32 devices in a mesh: ep: 8 (over z, x), tp: 4 (over y, core).
Axes of the slice: x: 2, y: 2, z: 4, core: 2. Of those that a mesh axis runs over, the one named last changes fastest.
Arguments:
- projected_queries: bfloat16 [2048, 2048], P('ep', 'tp'), may hold values from -245 to 245, as said below
- key_proj: bfloat16 [2048, 512], P('ep', 'tp'), may hold values from -6.2 to 6.2
- projected_values: bfloat16 [2048, 512], P('ep', 'tp'), may hold values from -24 to 24
- head_sink_logits: float32 [32], P('tp'), may hold values from 1 to 6
- out_weight: bfloat16 [2048, 4096], P('tp'), may hold values from -0.125 to 0.125
- expert_input: bfloat16 [1024, 4096], P('ep'), may hold values from -6 to 6
- norm_gain: float32 [4096], replicated, may hold values from 0.1 to 1.9
- routing: int32 [1024, 4], P('ep'), may hold values from 0 to 7, all different within a row; in each aligned block of 128 rows (0 to 127, 128 to 255, ...) at most 96 rows name the same one
- route_weight: float32 [1024, 4], P('ep'), may hold values from 0.1 to 1
- gate_weight: bfloat16 [8, 4096, 1024], P('ep', None, 'tp'), may hold values from -0.27929688 to 0.27929688
- up_weight: bfloat16 [8, 4096, 1024], P('ep', None, 'tp'), may hold values from -0.27929688 to 0.27929688
- down_weight: bfloat16 [8, 1024, 4096], P('ep', 'tp'), may hold values from -0.046875 to 0.046875
Outputs:
- mixer_output: bfloat16 [2048, 4096], P(('ep', 'tp'))
- expert_output: bfloat16 [1024, 4096], P('ep', 'tp')
The draws below stay inside these ranges and needn't reach their ends.
Inputs may be any that keep to these rules, and one draw needn't show every extreme that they name: `projected_queries`: in the hidden draw some queries nearly equal a large multiple of a nearby key. `routing`: each row names 4 different experts; among the rows of one device (aligned blocks of 128 rows) no expert is named more than 96 times, a bound that some block reaches.
All inputs are finite; a program needn't handle non-finite values.
Results may differ from the reference program's by a relative error of at most 0.014.
Values may be sent and summed in bfloat16 or wider, within the bound.
A program may use at most 128 MiB of HBM per device.

```python
import math
import jax
import jax.numpy as jnp
import numpy as np
from jax import lax

D = 4096
QUERY_HEADS = 32
KEY_VALUE_HEADS = 8
HEAD_SIZE = 64
WINDOW_KEYS = 128
FF = 1024
TOPK = 4
TOK_B_DEV = 128
EXPERTS = 8
CAP = 96
ATTENTION_TOKENS = 2048
TOKENS_B = 1024
N_EP = 8
N_TP = 4


def plant_pair(key):
    base = jax.random.fold_in(key, 17)
    leading_key, following_key = jax.random.split(base, 2)
    sampled_keys = jnp.clip(jax.random.normal(following_key, (ATTENTION_TOKENS, KEY_VALUE_HEADS, HEAD_SIZE), jnp.float32), -6.0, 6.0)
    query_vectors = jnp.clip(jax.random.normal(leading_key, (ATTENTION_TOKENS, KEY_VALUE_HEADS, QUERY_HEADS // KEY_VALUE_HEADS, HEAD_SIZE), jnp.float32), -6.0, 6.0)
    return (query_vectors.reshape(ATTENTION_TOKENS, QUERY_HEADS * HEAD_SIZE), sampled_keys.reshape(ATTENTION_TOKENS, KEY_VALUE_HEADS * HEAD_SIZE))


def draw_projected_queries(key, part):
    return plant_pair(key)[0].astype(jnp.bfloat16)


def draw_key_proj(key, part):
    return plant_pair(key)[1].astype(jnp.bfloat16)


def block_scale(own_key, extent, cuts, smallest, largest):
    factor_of, own = 1.0, jax.random.fold_in(own_key, 6)
    for dim, shards_of in cuts:
        draws = jnp.exp(jax.random.uniform(jax.random.fold_in(own, dim), (shards_of,), jnp.float32, smallest / len(cuts), largest / len(cuts)))
        factor_of = factor_of * jnp.repeat(draws, extent[dim] // shards_of).reshape([-1 if axis == dim else 1 for axis in range(len(extent))])
    return factor_of


def assign_block(key, own, number, rows, number_of, top, bound, skew):
    sequence = jax.random.permutation(key, number_of)
    heavy_load, common = shares(number_of, rows * top, bound, skew, True), shares(number_of, rows * top, bound, skew, False)
    places = jnp.arange(number_of)

    def named(tallies, rotation):
        used = int((tallies > 0).sum())
        fixed = max(1, used // 4)
        moved = fixed + (places - fixed + rotation * (used - fixed)) % max(1, number_of - fixed)
        return jnp.zeros((number_of,), jnp.int32).at[sequence[jnp.where(places < fixed, places, moved)]].set(jnp.asarray(tallies, jnp.int32))

    tallies = jnp.where(number % 4 == 0, named(heavy_load, number // 4), named(common, number - number // 4 - 1))
    mixed = jax.random.permutation(jax.random.fold_in(own, 3), number_of)
    giver, taker = mixed[0:number_of // 2 * 2:2], mixed[1:number_of // 2 * 2:2]
    room = jnp.minimum(tallies[giver] - 1, bound - tallies[taker]) // 2
    room = jnp.where((giver == sequence[0]) | (taker == sequence[0]) | (tallies[taker] == 0), 0, jnp.maximum(room, 0))
    moved = jax.random.randint(jax.random.fold_in(own, 4), (number_of // 2,), 0, 1 << 20) % (room + 1)
    tallies = tallies.at[giver].add(-moved).at[taker].add(moved)
    items = jnp.searchsorted(jnp.cumsum(tallies), jnp.arange(rows * top), side="right").astype(jnp.int32)
    table = items.reshape(top, rows).T
    table = table[jax.random.permutation(jax.random.fold_in(own, 1), rows)]
    rotation = jax.random.randint(jax.random.fold_in(own, 2), (rows, 1), 0, top)
    return jnp.take_along_axis(table, (jnp.arange(top)[None, :] + rotation) % top, axis=1)


def shares(number_of, total, limit, slope, full):
    loads = [(1 << 20) // math.isqrt(rank ** slope) + 1 for rank in range(1, number_of + 1)]
    largest = limit if full else min(limit, max(-(-total // number_of), total * loads[0] // sum(loads)))
    least = 1 if total - largest >= number_of - 1 else 0
    holding, surplus = [largest] + [least] * (number_of - 1), total - largest - least * (number_of - 1)
    while surplus > 0:
        free = [i for i in range(1, number_of) if holding[i] < largest] or [i for i in range(1, number_of) if holding[i] < limit]
        pool, remaining = sum([loads[i] for i in free]), surplus
        for i in free:
            more = min(limit - holding[i], max(1, remaining * loads[i] // pool), surplus)
            holding[i] = holding[i] + more
            surplus = surplus - more
    return np.array(holding)


def scatter_about(stream_key, shape, scale, bound, cuts=(), held_as=jnp.bfloat16):
    gain = block_scale(stream_key, shape, cuts, -0.22, 0.18) if cuts else 1.0
    drawn = jax.random.normal(stream_key, shape, jnp.float32) * scale * gain
    return jnp.minimum(jnp.maximum(drawn, -bound), bound).astype(held_as)


def setup_inputs(seed: int = 0) -> dict:
    arg_keys = jax.random.split(jax.random.key(seed), 13)
    projected_queries = draw_projected_queries(jax.random.fold_in(arg_keys[12], 71), 0)
    key_proj = draw_key_proj(jax.random.fold_in(arg_keys[12], 71), 0)
    projected_values = scatter_about(arg_keys[2], (ATTENTION_TOKENS, KEY_VALUE_HEADS * HEAD_SIZE), 4.0, 24.0, ((0, 8), (1, 4)))
    head_sink_logits = jnp.clip(1.0 + 5.0 * jax.random.uniform(arg_keys[3], (QUERY_HEADS,), jnp.float32) ** block_scale(arg_keys[3], (QUERY_HEADS,), ((0, 4),), -0.2, 0.2), 1.0, 6.0)
    out_weight = scatter_about(arg_keys[4], (QUERY_HEADS * HEAD_SIZE, D), (QUERY_HEADS * HEAD_SIZE) ** -0.5, 0.125, ((0, 4),))
    expert_input = scatter_about(arg_keys[5], (TOKENS_B, D), 1.0, 6.0, ((0, 8),))
    norm_gain = jnp.clip(1.0 + 0.18 * jax.random.normal(arg_keys[6], (D,), jnp.float32), 0.1, 1.9)
    routing_keys = jax.random.split(jax.random.fold_in(arg_keys[7], 1), TOKENS_B // TOK_B_DEV)
    routing_turns = jax.random.permutation(jax.random.fold_in(arg_keys[7], 3), TOKENS_B // TOK_B_DEV)
    routing = jax.vmap(lambda own, number: assign_block(jax.random.fold_in(arg_keys[7], 2), own, number, TOK_B_DEV, N_EP, TOPK, CAP, 2))(routing_keys, routing_turns).reshape((TOKENS_B, TOPK))
    route_weight = jnp.clip(jnp.exp(math.log(1.0) - 2.3025851 * jax.random.uniform(arg_keys[8], (TOKENS_B, TOPK), jnp.float32) ** block_scale(arg_keys[8], (TOKENS_B, TOPK), ((0, 8),), -0.2, 0.2)), 0.1, 1.0)
    gate_weight = scatter_about(arg_keys[9], (EXPERTS, D, FF), 0.046875, 0.27929688, ((0, 8), (2, 4)))
    up_weight = scatter_about(arg_keys[10], (EXPERTS, D, FF), 0.046875, 0.27929688, ((0, 8), (2, 4)))
    down_weight = scatter_about(arg_keys[11], (EXPERTS, FF, D), (16 * FF) ** -0.5, 0.046875, ((0, 8), (1, 4)))
    return {"projected_queries": projected_queries, "key_proj": key_proj, "projected_values": projected_values, "head_sink_logits": head_sink_logits, "out_weight": out_weight, "expert_input": expert_input, "norm_gain": norm_gain, "routing": routing, "route_weight": route_weight, "gate_weight": gate_weight, "up_weight": up_weight, "down_weight": down_weight}


EPS = 1e-06
CLAMP = 7.0
SLOPE = 1.702

def attend_single_head(kernel_inputs, permitted_mask):
    query_head, key_head, value_head, sink_head = kernel_inputs
    scores = jnp.einsum('nqgd,nsd->ngqs', query_head, key_head) * HEAD_SIZE ** (-0.5)
    scores = jnp.where(permitted_mask[:, None, :, :], scores, -jnp.inf)
    sink_col = sink_head[None, :, None, None]
    highest = jnp.maximum(lax.optimization_barrier(jnp.max(scores, axis=-1, keepdims=True)), sink_col)
    numerator = jnp.exp(scores - highest)
    denominator = lax.optimization_barrier(jnp.sum(numerator, axis=-1, keepdims=True)) + jnp.exp(sink_col - highest)
    weights = (numerator / denominator).astype(jnp.bfloat16)
    return jnp.einsum('ngqs,nsd->nqgd', weights.astype(jnp.float32), value_head.astype(jnp.float32))

def slot_targets(flat_ids, capacity):
    onehot = (flat_ids[:, None] == jnp.arange(N_EP, dtype=jnp.int32)[None, :]).astype(jnp.int32)
    rank_in = jnp.cumsum(onehot, axis=0) - 1
    slot_pos = lax.optimization_barrier(jnp.sum(rank_in * onehot, axis=1))
    return (flat_ids * capacity + slot_pos).astype(jnp.int32)

def reference(projected_queries, key_proj, projected_values, head_sink_logits, out_weight, expert_input, norm_gain, routing, route_weight, gate_weight, up_weight, down_weight):
    total = projected_queries.shape[0]
    count_of_blocks = total // WINDOW_KEYS
    heads_per_group = QUERY_HEADS // KEY_VALUE_HEADS
    query_vectors = projected_queries.astype(jnp.float32).reshape(count_of_blocks, WINDOW_KEYS, KEY_VALUE_HEADS, heads_per_group, HEAD_SIZE)
    blank_rows = jnp.zeros((WINDOW_KEYS, KEY_VALUE_HEADS * HEAD_SIZE), jnp.bfloat16)
    padded_keys = jnp.concatenate([blank_rows, key_proj], axis=0).astype(jnp.float32)
    padded_values = jnp.concatenate([blank_rows, projected_values], axis=0)
    window_keys = jnp.concatenate([padded_keys[:-WINDOW_KEYS].reshape(count_of_blocks, WINDOW_KEYS, KEY_VALUE_HEADS, HEAD_SIZE), padded_keys[WINDOW_KEYS:].reshape(count_of_blocks, WINDOW_KEYS, KEY_VALUE_HEADS, HEAD_SIZE)], axis=1)
    window_values = jnp.concatenate([padded_values[:-WINDOW_KEYS].reshape(count_of_blocks, WINDOW_KEYS, KEY_VALUE_HEADS, HEAD_SIZE), padded_values[WINDOW_KEYS:].reshape(count_of_blocks, WINDOW_KEYS, KEY_VALUE_HEADS, HEAD_SIZE)], axis=1)
    block_ids = jnp.arange(count_of_blocks)[:, None, None] * WINDOW_KEYS
    query_pos = block_ids + jnp.arange(WINDOW_KEYS)[None, :, None] + WINDOW_KEYS
    key_pos = block_ids + jnp.arange(2 * WINDOW_KEYS)[None, None, :]
    permitted_mask = (key_pos <= query_pos) & (query_pos - key_pos < WINDOW_KEYS) & (key_pos >= WINDOW_KEYS)
    head_outputs = lax.map(lambda kernel_inputs: attend_single_head(kernel_inputs, permitted_mask), (query_vectors.transpose(2, 0, 1, 3, 4), window_keys.transpose(2, 0, 1, 3), window_values.transpose(2, 0, 1, 3), head_sink_logits.reshape(KEY_VALUE_HEADS, heads_per_group)))
    attended = head_outputs.transpose(1, 2, 0, 3, 4).reshape(total, QUERY_HEADS * HEAD_SIZE).astype(jnp.bfloat16)
    head_share = QUERY_HEADS * HEAD_SIZE // N_TP
    summed = jnp.zeros((total, D), jnp.float32)
    for group in range(N_TP):
        partial_value = jnp.dot(attended[:, group * head_share:(group + 1) * head_share], out_weight[group * head_share:(group + 1) * head_share], preferred_element_type=jnp.float32).astype(jnp.bfloat16)
        summed = summed + lax.optimization_barrier(partial_value).astype(jnp.float32)
    mixer_output = summed.astype(jnp.bfloat16)
    capacity = CAP
    widened = expert_input.astype(jnp.float32)
    normed = (widened * lax.rsqrt(lax.optimization_barrier(jnp.mean(widened * widened, axis=-1, keepdims=True)) + EPS) * norm_gain[None, :]).astype(jnp.bfloat16)
    per_source = TOK_B_DEV * TOPK
    flat_ids = routing.reshape(N_EP, per_source).astype(jnp.int32)
    target = jax.vmap(lambda id_row: slot_targets(id_row, capacity))(flat_ids)
    tok_ids = (jnp.arange(per_source) // TOPK).astype(jnp.int32)
    slot_tok = jax.vmap(lambda tgt_row: jnp.full((N_EP * capacity,), TOK_B_DEV, jnp.int32).at[tgt_row].set(tok_ids))(target)
    extended = jnp.concatenate([normed.reshape(N_EP, TOK_B_DEV, D), jnp.zeros((N_EP, 1, D), jnp.bfloat16)], axis=1)

    def run_expert(expert_id):
        picks = lax.dynamic_slice_in_dim(slot_tok, expert_id * capacity, capacity, 1)
        expert_rows = jax.vmap(lambda block_rows, pick_row: jnp.take(block_rows, pick_row, axis=0))(extended, picks)
        expert_rows = expert_rows.reshape(N_EP * capacity, D)
        gate_pre = jnp.dot(expert_rows, gate_weight[expert_id], preferred_element_type=jnp.float32)
        up_pre = jnp.dot(expert_rows, up_weight[expert_id], preferred_element_type=jnp.float32)
        gate_cut = jnp.minimum(gate_pre, CLAMP)
        activated = ((jnp.clip(up_pre, -CLAMP, CLAMP) + 1.0) * gate_cut * jax.nn.sigmoid(SLOPE * gate_cut)).astype(jnp.bfloat16)
        return jnp.dot(activated, down_weight[expert_id], preferred_element_type=jnp.float32).astype(jnp.bfloat16)
    results = lax.map(run_expert, jnp.arange(N_EP, dtype=jnp.int32))
    source = jnp.arange(N_EP, dtype=jnp.int32)[:, None]
    slot_of = target - flat_ids * capacity
    gather_at = ((flat_ids * N_EP + source) * capacity + slot_of).astype(jnp.int32)
    picked = jnp.take(results.reshape(-1, D), gather_at.reshape(-1), axis=0).astype(jnp.float32)
    picked = picked.reshape(N_EP * TOK_B_DEV, TOPK, D)
    expert_output = lax.optimization_barrier(jnp.sum(picked * route_weight[:, :, None], axis=1)).astype(jnp.bfloat16)
    return (mixer_output, expert_output)
```

```python
import types

import jax
import jax.numpy as jnp
from jax import lax
from jax.experimental import pallas as pl
from jax.experimental.pallas import tpu as pltpu
from jax.sharding import PartitionSpec as P

D = 4096
HEAD_SIZE = 64
WINDOW_KEYS = 128
TOPK = 4


EPS = 1e-06
CLAMP = 7.0
SLOPE = 1.702


def passed_along(block, axis, distance):
    devices = range(lax.axis_size(axis))
    route = [(i - distance, i) for i in devices if i - distance in devices]
    return lax.ppermute(block, axis, route)


LINE = 4
SLOTS = 96
LONE = 4
EARLY = 5
MIXED_CUTS = 4
MESH = pl.DeviceIdType.MESH

NAMES = (
    "token_hbm", "gain_hbm", "routing_hbm", "route_weight_hbm", "query_hbm", "key_hbm",
    "value_hbm", "sink_hbm", "project_hbm", "gate_hbm", "up_hbm", "down_hbm", "mixer", "out",
    "token", "gain", "routing", "route_weight", "query", "key", "value", "sink", "own", "dense",
    "packed", "aside", "both_weights", "down", "project", "halo", "attended", "mixed",
    "mixed_core", "mixed_pair", "shares", "ranks", "hot", "slot_weight", "active", "results",
    "pair", "side", "line_out", "line_in", "last", "final", "mixer_kept", "out_kept", "keep_sem", "load_sem", "halo_send", "halo_recv",
    "mixed_core_send", "mixed_core_recv", "mixed_pair_send", "mixed_pair_recv", "share_send",
    "share_recv", "own_send", "onward_send", "along_recv", "across_send", "across_recv",
    "partner_send", "partner_recv", "core_send", "core_recv", "down_send", "down_recv",
    "active_send", "active_recv", "pair_send", "pair_recv", "side_send", "side_recv", "line_send",
    "line_recv", "last_send", "last_recv",
)


def chosen(z, values):
    result = jnp.int32(values[0])
    for place in range(1, LINE):
        result = jnp.where(z == place, jnp.int32(values[place]), result)
    return result


def nearest_first(place):
    return sorted(range(LINE), key=lambda other: (abs(other - place), abs(2 * other - LINE + 1)))


def sizes_of(width):
    quarter = width // 4
    lone = width * LONE // 32
    both = (width - 4 * lone) // 2
    early = width * EARLY // 32
    return quarter, lone, both, early, 2 * quarter - early


def parts_of(lone, both):
    return (0, lone), (lone, both // 2), (lone + both // 2, both // 2)


def chunks_of(quarter, early):
    late, first = quarter - early, (early + 128) // 256 * 128
    return (quarter, late), (early, late), (0, first), (first, early - first)


def layer_kernel(*refs):
    r = types.SimpleNamespace(**dict(zip(NAMES, refs)))
    e, t = lax.axis_index("ep"), lax.axis_index("tp")
    z, x, y, c = e // 2, e % 2, t // 2, t % 2
    tokens, width = r.token_hbm.shape
    quarter, lone, both, early, carried = sizes_of(width)
    held = lone + both
    hidden = r.gate_hbm.shape[1]
    sibling, partner, beside = (e, y * 2 + 1 - c), (e, (1 - y) * 2 + c), (z * 2 + 1 - x, t)
    at_end = (z == 0) | (z == LINE - 1)
    at_middle = (z > 0) & (z < LINE - 1)
    near = [chosen(z, [nearest_first(place)[j] for place in range(LINE)]) for j in range(LINE)]

    def copy(src, dst, send, recv, to):
        return pltpu.make_async_remote_copy(
            src_ref=src, dst_ref=dst, send_sem=send, recv_sem=recv, device_id=to, device_id_type=MESH
        )

    def aligned(start, length):
        return pl.ds(pl.multiple_of(start, 128), length)

    def lone_of(row, core):
        return aligned(row * (width - 2 * lone) + core * lone, lone)

    def both_of(core):
        return aligned(2 * lone + core * both, both)

    sections = [
        (lone_of(y, c), 0, lone),
        (both_of(c), lone, both),
        (lone_of(y, 1 - c), held, lone),
        (both_of(1 - c), held + lone, both),
        (lone_of(1 - y, c), 2 * held, lone),
        (lone_of(1 - y, 1 - c), 2 * held + lone, lone),
    ]
    mine, theirs = (y * 2 + c) * quarter, ((1 - y) * 2 + c) * quarter

    def result_columns(core):
        own, other = (y * 2 + core) * quarter, ((1 - y) * 2 + core) * quarter
        return [
            (aligned(own, quarter), 0, quarter),
            (aligned(other + early, quarter - early), quarter, quarter - early),
            (aligned(other, early), carried, early),
        ]

    pieces = [
        (r.routing_hbm, r.routing), (r.route_weight_hbm, r.route_weight), (r.token_hbm, r.token),
        (r.gain_hbm, r.gain), (r.sink_hbm, r.sink), (r.query_hbm, r.query), (r.key_hbm, r.key),
        (r.value_hbm, r.value), (r.project_hbm, r.project),
    ]
    small = len(pieces) - 1
    for columns, place, length in sections:
        for number, weights in enumerate((r.gate_hbm, r.up_hbm)):
            pieces.append(
                (
                    weights.at[columns, :],
                    r.both_weights.at[pl.ds(place, length), pl.ds(number * hidden, hidden)],
                )
            )
    for columns, place, length in result_columns(c):
        pieces.append((r.down_hbm.at[:, columns], r.down.at[pl.ds(0, hidden), pl.ds(place, length)]))
    loads = [
        pltpu.make_async_copy(src, dst, r.load_sem.at[place]) for place, (src, dst) in enumerate(pieces)
    ]
    for load in loads[:small]:
        load.start()

    barrier = pltpu.get_barrier_semaphore()
    for step in range(1, 2 * LINE):
        pl.semaphore_signal(
            barrier, inc=1, device_id=((e + step) % (2 * LINE), t), device_id_type=MESH
        )
    for other in (sibling, partner):
        pl.semaphore_signal(barrier, inc=1, device_id=other, device_id_type=MESH)

    for load in loads[:4]:
        load.wait()
    for load in loads[small:]:
        load.start()
    widened = r.token[...].astype(jnp.float32)
    scale = lax.rsqrt(jnp.mean(widened * widened, axis=-1, keepdims=True) + EPS)
    r.own[...] = (widened * scale * r.gain[...]).astype(jnp.bfloat16)

    expert = lax.broadcasted_iota(jnp.int32, (2 * LINE, tokens), 0)
    named = jnp.zeros((2 * LINE, tokens), jnp.float32)
    for k in range(TOPK):
        named = named + jnp.where(expert == r.routing[k : k + 1], r.route_weight[k : k + 1], 0.0)
    r.shares[e] = named

    ahead = (
        lax.broadcasted_iota(jnp.int32, (tokens, tokens), 0)
        <= lax.broadcasted_iota(jnp.int32, (tokens, tokens), 1)
    ).astype(jnp.float32)
    slot = (lax.broadcasted_iota(jnp.int32, (SLOTS, tokens), 0) + 1).astype(jnp.float32)

    def ranked(block):
        routed = jnp.where(r.shares[block] > 0.0, 1.0, 0.0)
        r.ranks[block] = jnp.dot(routed, ahead, preferred_element_type=jnp.float32)

    def one_hot(block, expert):
        weight = r.shares[block, pl.ds(expert, 1), :]
        here = (r.ranks[block, pl.ds(expert, 1), :] == slot) & (weight > 0.0)
        return jnp.where(here, 1.0, 0.0), jnp.sum(jnp.where(here, weight, 0.0), axis=1, keepdims=True)

    def keep_weight(at, half, found):
        r.slot_weight[at, half * SLOTS : (half + 1) * SLOTS, :] = jnp.broadcast_to(found, (SLOTS, 128))

    def prepare(at):
        ranked(at * 2 + x)
        hot, found = one_hot(at * 2 + x, e)
        keep_weight(at, 0, found)
        r.hot[at, 0:SLOTS, :] = hot.astype(jnp.bfloat16)
        r.hot[at, SLOTS : 2 * SLOTS, :] = one_hot(at * 2 + x, z * 2 + 1 - x)[0].astype(jnp.bfloat16)

    def prepare_other(at):
        ranked(at * 2 + 1 - x)
        keep_weight(at, 1, one_hot(at * 2 + 1 - x, e)[1])

    prepare(z)
    for load in loads[4:small]:
        load.wait()
    pl.semaphore_wait(barrier, 2 * LINE + 1)

    parts = parts_of(lone, both)
    start_of_both = 2 * lone + c * both
    own_columns = (
        sections[0][0], aligned(start_of_both, both // 2), aligned(start_of_both + both // 2, both // 2)
    )

    def rows_of(half):
        return pl.ds(half * SLOTS, SLOTS)

    def own_along(up, part):
        start, length = parts[part]
        return copy(
            r.own.at[:, own_columns[part]], r.dense.at[z, :, pl.ds(start, length)],
            r.own_send.at[up, part], r.along_recv.at[z, part], (e + 4 * up - 2, t),
        )

    def onward(at, part):
        start, length = parts[part]
        view = r.dense.at[at, :, pl.ds(start, length)]
        to = (jnp.where(at < z, e + 2, e - 2), t)
        return copy(view, view, r.onward_send.at[at, part], r.along_recv.at[at, part], to)

    def across(at, part):
        start, length = parts[part]
        return copy(
            r.aside.at[at, :, pl.ds(start, length)],
            r.packed.at[at, rows_of(1), pl.ds(start, length)],
            r.across_send.at[at, part], r.across_recv.at[at, part], beside,
        )

    def to_partner(at, half):
        return copy(
            r.packed.at[at, rows_of(half), pl.ds(0, lone)],
            r.packed.at[at, rows_of(half), pl.ds(2 * held, lone)],
            r.partner_send.at[at, half], r.partner_recv.at[at, half], partner,
        )

    core_parts = [(start, held + start, length) for start, length in parts]
    core_parts.append((2 * held, 2 * held + lone, lone))

    def to_sibling(at, half, kind):
        start, landing, length = core_parts[kind]
        return copy(
            r.packed.at[at, rows_of(half), pl.ds(start, length)],
            r.packed.at[at, rows_of(half), pl.ds(landing, length)],
            r.core_send.at[at, half, kind], r.core_recv.at[at, half, kind], sibling,
        )

    def share_copy(step):
        to = (e + step) % (2 * LINE)
        return copy(r.shares.at[e], r.shares.at[e], r.share_send.at[step], r.share_recv.at[e], (to, t))

    def share_in(block):
        return copy(
            r.shares.at[block], r.shares.at[block], r.share_send.at[0], r.share_recv.at[block], beside
        )

    def own_along_start(part):
        @pl.when(z < LINE - 1)
        def _():
            own_along(1, part).start()

        @pl.when(z > 0)
        def _():
            own_along(0, part).start()

    def pack_aside(part):
        start, length = parts[part]
        found = jnp.dot(
            r.hot[z, SLOTS : 2 * SLOTS, :], r.own[:, own_columns[part]],
            preferred_element_type=jnp.float32,
        )
        r.aside[z, :, start : start + length] = found.astype(jnp.bfloat16)
        across(z, part).start()

    queries = r.query_hbm.shape[0]

    def halo_copy(which):
        src = (r.key, r.value)[which].at[pl.ds(queries - WINDOW_KEYS, WINDOW_KEYS)]
        to = ((e + 1) % (2 * LINE), t)
        return copy(src, r.halo.at[which], r.halo_send.at[which], r.halo_recv.at[which], to)

    @pl.when(e < 2 * LINE - 1)
    def _():
        halo_copy(0).start()
        halo_copy(1).start()

    @pl.when(e == 0)
    def _():
        r.halo[...] = jnp.zeros_like(r.halo)

    own_along_start(0)
    for step in range(1, 2 * LINE):
        share_copy(step).start()
    pack_aside(0)
    for part in range(1, len(parts)):
        own_along_start(part)
        pack_aside(part)

    def down_copy(number):
        columns, place, length = result_columns(1 - c)[number]
        return copy(
            r.down_hbm.at[:, columns], r.down.at[pl.ds(hidden, hidden), pl.ds(place, length)],
            r.down_send.at[number], r.down_recv.at[number], sibling,
        )

    for number in range(3):
        down_copy(number).start()

    for columns, place, length in sections:
        found = jnp.dot(r.hot[z, 0:SLOTS, :], r.own[:, columns], preferred_element_type=jnp.float32)
        r.packed[z, 0:SLOTS, place : place + length] = found.astype(jnp.bfloat16)

    kv_heads = r.key_hbm.shape[1] // HEAD_SIZE
    group = r.query_hbm.shape[1] // HEAD_SIZE // kv_heads
    span = queries // 4
    here = lax.broadcasted_iota(jnp.int32, (WINDOW_KEYS, 2 * WINDOW_KEYS), 0)
    there = lax.broadcasted_iota(jnp.int32, (WINDOW_KEYS, 2 * WINDOW_KEYS), 1)

    def attend(number, kv):
        begin = number * WINDOW_KEYS
        permitted = (there > here) & (there <= here + WINDOW_KEYS)
        if number == 0:
            permitted = permitted & ((there >= WINDOW_KEYS) | (e > 0))
        lanes = slice(kv * HEAD_SIZE, (kv + 1) * HEAD_SIZE)
        if number == 0:
            keys = jnp.concatenate([r.halo[0][:, lanes], r.key[0:WINDOW_KEYS, lanes]], axis=0)
            values = jnp.concatenate([r.halo[1][:, lanes], r.value[0:WINDOW_KEYS, lanes]], axis=0)
        else:
            keys = r.key[begin - WINDOW_KEYS : begin + WINDOW_KEYS, lanes]
            values = r.value[begin - WINDOW_KEYS : begin + WINDOW_KEYS, lanes]
        for member in range(group):
            head = kv * group + member
            columns = slice(head * HEAD_SIZE, (head + 1) * HEAD_SIZE)
            scores = lax.dot_general(
                r.query[begin : begin + WINDOW_KEYS, columns],
                keys,
                (((1,), (1,)), ((), ())),
                preferred_element_type=jnp.float32,
            ) * HEAD_SIZE ** (-0.5)
            scores = jnp.where(permitted, scores, -jnp.inf)
            sink = r.sink[head]
            highest = jnp.maximum(jnp.max(scores, axis=-1, keepdims=True), sink)
            numerator = jnp.exp(scores - highest)
            denominator = jnp.sum(numerator, axis=-1, keepdims=True) + jnp.exp(sink - highest)
            weights = (numerator / denominator).astype(jnp.bfloat16)
            found = jnp.dot(weights, values, preferred_element_type=jnp.float32)
            r.attended[begin : begin + WINDOW_KEYS, columns] = found.astype(jnp.bfloat16)

    def halo_wait():
        @pl.when(e > 0)
        def _():
            halo_copy(0).wait_recv()
            halo_copy(1).wait_recv()

    def mixed_core(half):
        at = pl.multiple_of((half * 2 + 1 - c) * span, 16)
        return copy(
            r.mixed.at[pl.ds(at, span)], r.mixed_core.at[half],
            r.mixed_core_send.at[half], r.mixed_core_recv.at[half], sibling,
        )

    cut = span // MIXED_CUTS

    def mixed_pair(number):
        at = pl.multiple_of(((1 - y) * 2 + c) * span + number * cut, 16)
        return copy(
            r.mixed.at[pl.ds(at, cut)], r.mixed_pair.at[pl.ds(number * cut, cut)],
            r.mixed_pair_send.at[number], r.mixed_pair_recv.at[number], partner,
        )

    def mixed_rows(half):
        return pl.ds(pl.multiple_of((half * 2 + c) * span, 16), span)

    def mix():
        loads[small].wait()
        for place in range(0, width, quarter):
            columns = slice(place, place + quarter)
            r.mixed[:, columns] = jnp.dot(
                r.attended[...], r.project[:, columns], preferred_element_type=jnp.float32
            ).astype(jnp.bfloat16)
        for half in range(2):
            mixed_core(half).start()

    def mix_onward():
        for half in range(2):
            mixed_core(half).wait_recv()
            total = r.mixed[mixed_rows(half), :].astype(jnp.float32)
            r.mixed[mixed_rows(half), :] = (
                total + r.mixed_core[half].astype(jnp.float32)
            ).astype(jnp.bfloat16)

    def forward(k, part):
        onward(near[k], part).wait_recv()
        onward(near[k], part).start()

    def forward_middle(k, part):
        @pl.when(at_middle)
        def _():
            forward(k, part)

    def wait_end(k, part):
        @pl.when(at_end)
        def _():
            onward(near[k], part).wait_recv()

    def pack(k, part):
        at = near[k]
        start, length = parts[part]
        found = jnp.dot(
            r.hot[at], r.dense[at, :, start : start + length], preferred_element_type=jnp.float32
        ).astype(jnp.bfloat16)
        r.aside[at, :, start : start + length] = found[SLOTS : 2 * SLOTS]
        across(at, part).start()
        r.packed[at, 0:SLOTS, start : start + length] = found[0:SLOTS]
        if part == 0:
            to_partner(at, 0).start()
        to_sibling(at, 0, part).start()

    def take_across(k, part):
        at = near[k]
        across(at, part).wait_recv()
        if part == 0:
            to_partner(at, 1).start()
        to_sibling(at, 1, part).start()

    def take_partner(k, half):
        to_partner(near[k], half).wait_recv()
        to_sibling(near[k], half, len(parts)).start()

    def get_ready(k):
        share_in(near[k] * 2 + x).wait_recv()
        prepare(near[k])

    def get_other_ready(k):
        share_in(near[k] * 2 + 1 - x).wait_recv()
        prepare_other(near[k])

    def active_copy(at):
        return copy(
            r.active.at[at, :, pl.ds(0, hidden)], r.active.at[at, :, pl.ds(hidden, hidden)],
            r.active_send.at[at], r.active_recv.at[at], sibling,
        )

    def enter(k):
        at = near[k]
        for half in (1, 0) if k else (1,):
            for kind in range(len(core_parts)):
                to_sibling(at, half, kind).wait_recv()
        pre = jnp.dot(r.packed[at], r.both_weights[...], preferred_element_type=jnp.float32)
        gate_cut = jnp.minimum(pre[:, 0:hidden], CLAMP)
        up_pre = pre[:, hidden : 2 * hidden]
        r.active[at, :, 0:hidden] = (
            (jnp.clip(up_pre, -CLAMP, CLAMP) + 1.0) * gate_cut * jax.nn.sigmoid(SLOPE * gate_cut)
        ).astype(jnp.bfloat16)
        active_copy(at).start()

    late = quarter - early
    chunks = chunks_of(quarter, early)

    def pair_copy(at, half):
        return copy(
            r.results.at[at, rows_of(half), pl.ds(carried, early)], r.pair.at[at, rows_of(half), :],
            r.pair_send.at[at, half], r.pair_recv.at[at, half], partner,
        )

    def side_copy(at, chunk):
        start, length = chunks[chunk]
        return copy(
            r.results.at[at, rows_of(1), pl.ds(start, length)], r.side.at[at, :, pl.ds(start, length)],
            r.side_send.at[at, chunk], r.side_recv.at[at, chunk], beside,
        )

    def leave(k):
        at = near[k]
        active_copy(at).wait_recv()

        def finish(start, length):
            found = jnp.dot(
                r.active[at], r.down[:, start : start + length], preferred_element_type=jnp.float32
            )
            r.results[at, :, start : start + length] = (found * r.slot_weight[at][:, 0:1]).astype(
                jnp.bfloat16
            )

        finish(carried, early)
        if k > 1:
            send_pair(k, 1)
            send_pair(k, 0)
        for chunk in range(2):
            finish(*chunks[chunk])
            if k:
                side_copy(at, chunk).start()
        finish(0, early)

    def send_pair(k, half):
        pair_copy(near[k], half).start()

    def send_side(k):
        side_copy(near[k], 0).start()
        side_copy(near[k], 1).start()

    def take_pair(k, half):
        at = near[k]
        pair_copy(at, half).wait_recv()
        rows = slice(half * SLOTS, (half + 1) * SLOTS)
        for chunk in range(2, len(chunks)):
            columns = slice(chunks[chunk][0], chunks[chunk][0] + chunks[chunk][1])
            total = r.results[at, rows, columns].astype(jnp.float32)
            r.results[at, rows, columns] = (
                total + r.pair[at, rows, columns].astype(jnp.float32)
            ).astype(jnp.bfloat16)
            if half:
                side_copy(at, chunk).start()

    def line_copy(way, at, chunk):
        start, length = chunks[chunk]
        to = (jnp.where(at > z, e + 2, e - 2), t)
        return copy(
            r.line_out.at[at, :, pl.ds(start, length)], r.line_in.at[way, at, :, pl.ds(start, length)],
            r.line_send.at[at, chunk], r.line_recv.at[way, at, chunk], to,
        )

    last = copy(r.line_out.at[z, :, pl.ds(quarter, late)], r.last, r.last_send, r.last_recv, partner)

    def line_step(k, chunk, middle):
        at = near[k]
        start, length = chunks[chunk]
        columns = slice(start, start + length)
        side_copy(at, chunk).wait_recv()
        both_sides = jnp.concatenate([r.results[at, 0:SLOTS, columns], r.side[at, :, columns]], axis=0)
        total = lax.dot_general(
            r.hot[at], both_sides, (((0,), (0,)), ((), ())), preferred_element_type=jnp.float32
        )
        if k:
            way = jnp.where(at > z, 0, 1)
            ways = (way,) if middle else ()
        elif middle:
            ways = (0, 1)
        else:
            ways = (jnp.where(z == 0, 1, 0),)
        for way in ways:
            line_copy(way, at, chunk).wait_recv()
            total = total + r.line_in[way, at, :, columns].astype(jnp.float32)
        if k or chunk == 0:
            r.line_out[at, :, columns] = total.astype(jnp.bfloat16)
            if k:
                line_copy(way, at, chunk).start()
            else:
                last.start()
        elif chunk == 1:
            r.final[...] = total
        else:
            r.out_kept[:, columns] = total.astype(jnp.bfloat16)
            keep_out(chunk).start()

    def arrive(k, part):
        wait_end(k, part)
        if k == 1:
            forward_middle(1, part)
        if k < LINE - 1:
            forward_middle(k + 1, part)

    def send_mixed(number):
        mixed_pair(number).start()

    def finish_mixed():
        for number in range(MIXED_CUTS):
            mixed_pair(number).wait_recv()
        total = r.mixed[mixed_rows(y), :].astype(jnp.float32)
        r.mixer_kept[...] = (total + r.mixed_pair[...].astype(jnp.float32)).astype(jnp.bfloat16)
        keep_mixer.start()

    def at_places(which, *steps):
        @pl.when(which)
        def _():
            for step in steps:
                step[0](*step[1:])

    def end_lines(k, *which):
        at_places(at_end, *[(line_step, k, chunk, False) for chunk in which])

    def middle_lines(k, *which):
        at_places(at_middle, *[(line_step, k, chunk, True) for chunk in which])

    keep_mixer = pltpu.make_async_copy(r.mixer_kept, r.mixer, r.keep_sem.at[0])

    def keep_out(chunk):
        start, length = chunks[chunk]
        view = pl.ds(start, length)
        return pltpu.make_async_copy(r.out_kept.at[:, view], r.out.at[:, view], r.keep_sem.at[chunk])

    def drain_dispatch():
        for part in range(len(parts)):
            @pl.when(z < LINE - 1)
            def _():
                own_along(1, part).wait_send()

            @pl.when(z > 0)
            def _():
                own_along(0, part).wait_send()

            @pl.when(at_middle)
            def _():
                for k in range(1, LINE):
                    onward(near[k], part).wait_send()

        @pl.when(e < 2 * LINE - 1)
        def _():
            halo_copy(0).wait_send()
            halo_copy(1).wait_send()

        for step in range(1, 2 * LINE):
            share_copy(step).wait_send()
        for number in range(3):
            down_copy(number).wait_send()
        for half in range(2):
            mixed_core(half).wait_send()
        for k in range(LINE):
            at = near[k]
            for part in range(len(parts)):
                across(at, part).wait_send()
            for half in (0, 1) if k else (1,):
                to_partner(at, half).wait_send()
                for kind in range(len(core_parts)):
                    to_sibling(at, half, kind).wait_send()
            active_copy(at).wait_send()

    def drain_return():
        for number in range(MIXED_CUTS):
            mixed_pair(number).wait_send()
        for k in range(LINE):
            for half in range(2):
                pair_copy(near[k], half).wait_send()
            for chunk in range(len(chunks)):
                side_copy(near[k], chunk).wait_send()

    attend(1, 0)
    attend(1, 1)
    take_across(0, 0)
    get_other_ready(0)
    get_ready(1)
    arrive(1, 0)
    pack(1, 0)
    halo_wait()
    attend(0, 0)
    attend(0, 1)
    take_across(0, 1)
    mix()
    arrive(1, 1)
    pack(1, 1)
    take_partner(0, 1)
    take_across(0, 2)
    mix_onward()
    arrive(1, 2)
    pack(1, 2)
    take_across(1, 0)
    send_mixed(0)
    get_other_ready(1)
    get_ready(2)
    for load in loads[small + 1 :]:
        load.wait()
    enter(0)
    take_partner(1, 0)
    take_across(1, 1)
    arrive(2, 0)
    pack(2, 0)
    for number in range(3):
        down_copy(number).wait_recv()
    leave(0)
    take_partner(1, 1)
    take_across(1, 2)
    arrive(2, 1)
    pack(2, 1)
    take_across(2, 0)
    send_mixed(1)
    enter(1)
    arrive(2, 2)
    pack(2, 2)
    take_partner(2, 0)
    take_across(2, 1)
    leave(1)
    get_ready(3)
    get_other_ready(2)
    arrive(3, 0)
    pack(3, 0)
    send_pair(1, 1)
    take_partner(2, 1)
    take_across(2, 2)
    arrive(3, 1)
    pack(3, 1)
    end_lines(1, 0, 1)
    enter(2)
    take_across(3, 0)
    send_pair(1, 0)
    arrive(3, 2)
    pack(3, 2)
    leave(2)
    take_partner(3, 0)
    take_across(3, 1)
    take_pair(1, 1)
    take_partner(3, 1)
    get_other_ready(3)
    take_across(3, 2)
    take_pair(1, 0)
    enter(3)
    end_lines(2, 0, 1)
    leave(3)
    send_mixed(2)
    send_mixed(3)
    send_pair(0, 1)
    send_pair(0, 0)
    take_pair(2, 1)
    end_lines(1, 2, 3)
    take_pair(2, 0)
    middle_lines(1, 0, 1)
    end_lines(3, 0, 1)
    end_lines(2, 2, 3)
    take_pair(3, 1)
    send_side(0)
    take_pair(3, 0)
    middle_lines(3, 0, 1)
    middle_lines(1, 2, 3)
    middle_lines(2, 0, 1)
    end_lines(3, 2, 3)
    take_pair(0, 1)
    take_pair(0, 0)
    drain_dispatch()
    middle_lines(3, 2)
    middle_lines(2, 2)
    middle_lines(3, 3)
    middle_lines(2, 3)
    finish_mixed()
    middle_lines(0, 0, 1, 2, 3)
    end_lines(0, 0, 1, 2)
    drain_return()
    end_lines(0, 3)

    last.wait_recv()
    r.out_kept[:, early:quarter] = (r.final[...] + r.last[...].astype(jnp.float32)).astype(
        jnp.bfloat16
    )
    keep_out(1).start()
    last.wait_send()
    for k in range(1, LINE):
        for chunk in range(len(chunks)):
            line_copy(0, near[k], chunk).wait_send()
    keep_mixer.wait()
    for chunk in range(1, len(chunks)):
        keep_out(chunk).wait()


def layer_call(
    rows, gain, routing, route_weight, queries, keys, values, sinks, project, gate_one, up_one, down_one
):
    tokens, width = rows.shape
    quarter, lone, both, early, carried = sizes_of(width)
    parts, chunks = len(parts_of(lone, both)), len(chunks_of(quarter, early))
    blocks = 2 * LINE
    hidden = gate_one.shape[1]
    kept = jnp.bfloat16
    dma = pltpu.SemaphoreType.DMA
    span = queries.shape[0] // 4
    stays = pl.BlockSpec(memory_space=pl.ANY)
    scratch = dict(
        token=pltpu.VMEM(rows.shape, kept),
        gain=pltpu.VMEM(gain.shape, jnp.float32),
        routing=pltpu.VMEM(routing.shape, jnp.int32),
        route_weight=pltpu.VMEM(route_weight.shape, jnp.float32),
        query=pltpu.VMEM(queries.shape, kept),
        key=pltpu.VMEM(keys.shape, kept),
        value=pltpu.VMEM(values.shape, kept),
        sink=pltpu.SMEM(sinks.shape, jnp.float32),
        own=pltpu.VMEM((tokens, width), kept),
        dense=pltpu.VMEM((LINE, tokens, lone + both), kept),
        packed=pltpu.VMEM((LINE, 2 * SLOTS, width), kept),
        aside=pltpu.VMEM((LINE, SLOTS, lone + both), kept),
        both_weights=pltpu.VMEM((width, 2 * hidden), kept),
        down=pltpu.VMEM((2 * hidden, 2 * quarter), kept),
        project=pltpu.VMEM(project.shape, kept),
        halo=pltpu.VMEM((2, WINDOW_KEYS, keys.shape[1]), kept),
        attended=pltpu.VMEM(queries.shape, kept),
        mixed=pltpu.VMEM((queries.shape[0], width), kept),
        mixed_core=pltpu.VMEM((2, span, width), kept),
        mixed_pair=pltpu.VMEM((span, width), kept),
        shares=pltpu.VMEM((blocks, 8, tokens), jnp.float32),
        ranks=pltpu.VMEM((blocks, 8, tokens), jnp.float32),
        hot=pltpu.VMEM((LINE, 2 * SLOTS, tokens), kept),
        slot_weight=pltpu.VMEM((LINE, 2 * SLOTS, 128), jnp.float32),
        active=pltpu.VMEM((LINE, 2 * SLOTS, 2 * hidden), kept),
        results=pltpu.VMEM((LINE, 2 * SLOTS, 2 * quarter), kept),
        pair=pltpu.VMEM((LINE, 2 * SLOTS, early), kept),
        side=pltpu.VMEM((LINE, SLOTS, carried), kept),
        line_out=pltpu.VMEM((LINE, tokens, carried), kept),
        line_in=pltpu.VMEM((2, LINE, tokens, carried), kept),
        last=pltpu.VMEM((tokens, quarter - early), kept),
        final=pltpu.VMEM((tokens, quarter - early), jnp.float32),
        mixer_kept=pltpu.VMEM((span, width), kept),
        out_kept=pltpu.VMEM((tokens, quarter), kept),
        keep_sem=dma((chunks,)),
        load_sem=dma((24,)),
        halo_send=dma((2,)),
        halo_recv=dma((2,)),
        mixed_core_send=dma((2,)),
        mixed_core_recv=dma((2,)),
        mixed_pair_send=dma((MIXED_CUTS,)),
        mixed_pair_recv=dma((MIXED_CUTS,)),
        share_send=dma((blocks,)),
        share_recv=dma((blocks,)),
        own_send=dma((2, parts)),
        onward_send=dma((LINE, parts)),
        along_recv=dma((LINE, parts)),
        across_send=dma((LINE, parts)),
        across_recv=dma((LINE, parts)),
        partner_send=dma((LINE, 2)),
        partner_recv=dma((LINE, 2)),
        core_send=dma((LINE, 2, parts + 1)),
        core_recv=dma((LINE, 2, parts + 1)),
        down_send=dma((3,)),
        down_recv=dma((3,)),
        active_send=dma((LINE,)),
        active_recv=dma((LINE,)),
        pair_send=dma((LINE, 2)),
        pair_recv=dma((LINE, 2)),
        side_send=dma((LINE, chunks)),
        side_recv=dma((LINE, chunks)),
        line_send=dma((LINE, chunks)),
        line_recv=dma((2, LINE, chunks)),
        last_send=dma,
        last_recv=dma,
    )
    return pl.pallas_call(
        layer_kernel,
        out_shape=(
            jax.ShapeDtypeStruct((span, width), kept),
            jax.ShapeDtypeStruct((tokens, quarter), kept),
        ),
        in_specs=[stays] * 12,
        out_specs=(stays, stays),
        scratch_shapes=[scratch[name] for name in NAMES[14:]],
        compiler_params=pltpu.CompilerParams(
            collective_id=0, has_side_effects=True, vmem_limit_bytes=60 * 1024 * 1024
        ),
        cost_estimate=pl.CostEstimate(
            flops=8 * blocks * tokens * width * hidden,
            bytes_accessed=8 * width * hidden,
            transcendentals=0,
        ),
    )(rows, gain, routing, route_weight, queries, keys, values, sinks, project, gate_one, up_one, down_one)


def shards(
    projected_queries,
    key_proj,
    projected_values,
    head_sink_logits,
    out_weight,
    expert_input,
    norm_gain,
    routing,
    route_weight,
    gate_weight,
    up_weight,
    down_weight,
):
    token_rows = expert_input.shape[0]
    experts = lax.axis_size("ep")
    capacity = max(3 * token_rows * TOPK // (2 * experts), 2)
    col_share = D // lax.axis_size("tp")
    if (experts, lax.axis_size("tp")) == (2 * LINE, 4) and token_rows == 128:
        return layer_call(
            expert_input,
            norm_gain[None, :],
            routing.T,
            route_weight.T,
            projected_queries,
            key_proj,
            projected_values,
            head_sink_logits,
            out_weight,
            gate_weight[0],
            up_weight[0],
            down_weight[0],
        )
    widened = expert_input.astype(jnp.float32)
    normed = (
        widened
        * lax.rsqrt(jnp.mean(widened * widened, axis=-1, keepdims=True) + EPS)
        * norm_gain[None, :]
    ).astype(jnp.bfloat16)
    query_rows = projected_queries.shape[0]
    kv_heads = key_proj.shape[1] // HEAD_SIZE
    heads_per_group = projected_queries.shape[1] // HEAD_SIZE // kv_heads
    count_of_blocks = query_rows // WINDOW_KEYS
    prior_key, prior_value = passed_along(
        (key_proj[query_rows - WINDOW_KEYS :], projected_values[query_rows - WINDOW_KEYS :]),
        "ep",
        1,
    )
    key_all = jnp.concatenate([prior_key, key_proj], axis=0)
    value_all = jnp.concatenate([prior_value, projected_values], axis=0)
    window_keys = jnp.concatenate(
        [
            key_all[:-WINDOW_KEYS].reshape(count_of_blocks, WINDOW_KEYS, kv_heads, HEAD_SIZE),
            key_all[WINDOW_KEYS:].reshape(count_of_blocks, WINDOW_KEYS, kv_heads, HEAD_SIZE),
        ],
        axis=1,
    )
    window_values = jnp.concatenate(
        [
            value_all[:-WINDOW_KEYS].reshape(count_of_blocks, WINDOW_KEYS, kv_heads, HEAD_SIZE),
            value_all[WINDOW_KEYS:].reshape(count_of_blocks, WINDOW_KEYS, kv_heads, HEAD_SIZE),
        ],
        axis=1,
    )
    query_blocks = projected_queries.reshape(
        count_of_blocks, WINDOW_KEYS, kv_heads, heads_per_group, HEAD_SIZE
    )
    scores = jnp.einsum(
        "nqhgd,nshd->nhgqs", query_blocks, window_keys, preferred_element_type=jnp.float32
    ) * HEAD_SIZE ** (-0.5)
    offset = lax.axis_index("ep") * query_rows
    block_ids = jnp.arange(count_of_blocks)[:, None, None] * WINDOW_KEYS + offset
    query_pos = block_ids + jnp.arange(WINDOW_KEYS)[None, :, None]
    key_pos = block_ids - WINDOW_KEYS + jnp.arange(2 * WINDOW_KEYS)[None, None, :]
    permitted_mask = (key_pos <= query_pos) & (query_pos - key_pos < WINDOW_KEYS) & (key_pos >= 0)
    scores = jnp.where(permitted_mask[:, None, None, :, :], scores, -jnp.inf)
    sink_col = head_sink_logits.reshape(kv_heads, heads_per_group)[None, :, :, None, None]
    highest = jnp.maximum(jnp.max(scores, axis=-1, keepdims=True), sink_col)
    numerator = jnp.exp(scores - highest)
    denominator = jnp.sum(numerator, axis=-1, keepdims=True) + jnp.exp(sink_col - highest)
    weights = (numerator / denominator).astype(jnp.bfloat16)
    attended = jnp.einsum(
        "nhgqs,nshd->nqhgd", weights, window_values, preferred_element_type=jnp.float32
    )
    attended = attended.astype(jnp.bfloat16).reshape(
        query_rows, kv_heads * heads_per_group * HEAD_SIZE
    )
    mixer_output = lax.psum_scatter(
        jnp.dot(attended, out_weight, preferred_element_type=jnp.float32).astype(jnp.bfloat16),
        "tp",
        scatter_dimension=0,
        tiled=True,
    )
    flat_ids = routing.reshape(-1)
    onehot = (flat_ids[:, None] == jnp.arange(experts, dtype=jnp.int32)[None, :]).astype(jnp.int32)
    rank_in = jnp.cumsum(onehot, axis=0) - 1
    target = flat_ids * capacity + jnp.sum(rank_in * onehot, axis=1)
    tok_ids = jnp.arange(token_rows * TOPK) // TOPK
    slot_tok = jnp.full((experts * capacity,), token_rows, jnp.int32).at[target].set(tok_ids)
    gate_one = gate_weight[0]
    up_one = up_weight[0]
    own_cols = lax.dynamic_slice_in_dim(normed, lax.axis_index("tp") * col_share, col_share, 1)
    extended = jnp.concatenate([own_cols, jnp.zeros((1, col_share), jnp.bfloat16)], axis=0)
    outgoing = jnp.take(extended, slot_tok, axis=0).reshape(experts, capacity, col_share)
    arrived = lax.all_to_all(outgoing, "ep", split_axis=0, concat_axis=0, tiled=True).reshape(
        experts * capacity, col_share
    )
    portion = lax.all_gather(arrived, "tp", axis=1, tiled=True)
    gate_pre = jnp.dot(portion, gate_one, preferred_element_type=jnp.float32)
    up_pre = jnp.dot(portion, up_one, preferred_element_type=jnp.float32)
    gate_cut = jnp.minimum(gate_pre, CLAMP)
    activated = (
        (jnp.clip(up_pre, -CLAMP, CLAMP) + 1.0) * gate_cut * jax.nn.sigmoid(SLOPE * gate_cut)
    ).astype(jnp.bfloat16)
    partial_value = jnp.dot(activated, down_weight[0], preferred_element_type=jnp.float32)
    expert_result = lax.psum_scatter(
        partial_value.astype(jnp.bfloat16), "tp", scatter_dimension=1, tiled=True
    )
    returned = lax.all_to_all(
        expert_result.reshape(experts, capacity, col_share),
        "ep",
        split_axis=0,
        concat_axis=0,
        tiled=True,
    )
    picked = jnp.take(returned.reshape(experts * capacity, col_share), target, axis=0)
    picked = picked.astype(jnp.float32).reshape(token_rows, TOPK, col_share)
    expert_output = jnp.sum(picked * route_weight[:, :, None], axis=1).astype(jnp.bfloat16)
    return (mixer_output, expert_output)


def solution(mesh):
    placed = (
        P("ep", "tp"),
        P("ep", "tp"),
        P("ep", "tp"),
        P("tp"),
        P("tp", None),
        P("ep", None),
        P(),
        P("ep", None),
        P("ep", None),
        P("ep", None, "tp"),
        P("ep", None, "tp"),
        P("ep", "tp", None),
    )
    return jax.shard_map(
        shards,
        mesh=mesh,
        in_specs=placed,
        out_specs=(P(("ep", "tp"), None), P("ep", "tp")),
        check_vma=False,
    )
```

```python
import types

import jax
import jax.numpy as jnp
from jax import lax
from jax.experimental import pallas as pl
from jax.experimental.pallas import tpu as pltpu
from jax.sharding import PartitionSpec as P

D = 4096
HEAD_SIZE = 64
WINDOW_KEYS = 128
TOPK = 4


EPS = 1e-06
CLAMP = 7.0
SLOPE = 1.702


def passed_along(block, axis, distance):
    devices = range(lax.axis_size(axis))
    route = [(i - distance, i) for i in devices if i - distance in devices]
    return lax.ppermute(block, axis, route)


LINE = 4
SLOTS = 96
LONE = 4
EARLY = 5
MIXED_CUTS = 4
MESH = pl.DeviceIdType.MESH

NAMES = (
    "token_hbm", "gain_hbm", "routing_hbm", "route_weight_hbm", "query_hbm", "key_hbm",
    "value_hbm", "sink_hbm", "project_hbm", "gate_hbm", "up_hbm", "down_hbm", "mixer", "out",
    "token", "gain", "routing", "route_weight", "query", "key", "value", "sink", "own", "dense",
    "packed", "aside", "both_weights", "down", "project", "halo", "attended", "mixed",
    "mixed_core", "mixed_pair", "shares", "ranks", "hot", "slot_weight", "active", "results",
    "pair", "side", "line_out", "line_in", "last", "final", "load_sem", "halo_send", "halo_recv",
    "mixed_core_send", "mixed_core_recv", "mixed_pair_send", "mixed_pair_recv", "share_send",
    "share_recv", "own_send", "onward_send", "along_recv", "across_send", "across_recv",
    "partner_send", "partner_recv", "core_send", "core_recv", "down_send", "down_recv",
    "active_send", "active_recv", "pair_send", "pair_recv", "side_send", "side_recv", "line_send",
    "line_recv", "last_send", "last_recv",
)


def chosen(z, values):
    result = jnp.int32(values[0])
    for place in range(1, LINE):
        result = jnp.where(z == place, jnp.int32(values[place]), result)
    return result


def nearest_first(place):
    return sorted(range(LINE), key=lambda other: (abs(other - place), abs(2 * other - LINE + 1)))


def sizes_of(width):
    quarter = width // 4
    lone = width * LONE // 32
    both = (width - 4 * lone) // 2
    early = width * EARLY // 32
    return quarter, lone, both, early, 2 * quarter - early


def parts_of(lone, both):
    return (0, lone), (lone, both // 2), (lone + both // 2, both // 2)


def chunks_of(quarter, early):
    late, first = quarter - early, (early + 128) // 256 * 128
    return (quarter, late), (early, late), (0, first), (first, early - first)


def layer_kernel(*refs):
    r = types.SimpleNamespace(**dict(zip(NAMES, refs)))
    e, t = lax.axis_index("ep"), lax.axis_index("tp")
    z, x, y, c = e // 2, e % 2, t // 2, t % 2
    tokens, width = r.token_hbm.shape
    quarter, lone, both, early, carried = sizes_of(width)
    held = lone + both
    hidden = r.gate_hbm.shape[1]
    sibling, partner, beside = (e, y * 2 + 1 - c), (e, (1 - y) * 2 + c), (z * 2 + 1 - x, t)
    at_end = (z == 0) | (z == LINE - 1)
    at_middle = (z > 0) & (z < LINE - 1)
    near = [chosen(z, [nearest_first(place)[j] for place in range(LINE)]) for j in range(LINE)]

    def copy(src, dst, send, recv, to):
        return pltpu.make_async_remote_copy(
            src_ref=src, dst_ref=dst, send_sem=send, recv_sem=recv, device_id=to, device_id_type=MESH
        )

    def aligned(start, length):
        return pl.ds(pl.multiple_of(start, 128), length)

    def lone_of(row, core):
        return aligned(row * (width - 2 * lone) + core * lone, lone)

    def both_of(core):
        return aligned(2 * lone + core * both, both)

    sections = [
        (lone_of(y, c), 0, lone),
        (both_of(c), lone, both),
        (lone_of(y, 1 - c), held, lone),
        (both_of(1 - c), held + lone, both),
        (lone_of(1 - y, c), 2 * held, lone),
        (lone_of(1 - y, 1 - c), 2 * held + lone, lone),
    ]
    mine, theirs = (y * 2 + c) * quarter, ((1 - y) * 2 + c) * quarter

    def result_columns(core):
        own, other = (y * 2 + core) * quarter, ((1 - y) * 2 + core) * quarter
        return [
            (aligned(own, quarter), 0, quarter),
            (aligned(other + early, quarter - early), quarter, quarter - early),
            (aligned(other, early), carried, early),
        ]

    pieces = [
        (r.routing_hbm, r.routing), (r.route_weight_hbm, r.route_weight), (r.token_hbm, r.token),
        (r.gain_hbm, r.gain), (r.sink_hbm, r.sink), (r.query_hbm, r.query), (r.key_hbm, r.key),
        (r.value_hbm, r.value), (r.project_hbm, r.project),
    ]
    small = len(pieces) - 1
    for columns, place, length in sections:
        for number, weights in enumerate((r.gate_hbm, r.up_hbm)):
            pieces.append(
                (
                    weights.at[columns, :],
                    r.both_weights.at[pl.ds(place, length), pl.ds(number * hidden, hidden)],
                )
            )
    loads = [
        pltpu.make_async_copy(src, dst, r.load_sem.at[min(place, small + 1)])
        for place, (src, dst) in enumerate(pieces)
    ]
    for load in loads[:small]:
        load.start()

    down_loads = [
        pltpu.make_async_copy(
            r.down_hbm.at[:, columns], r.down.at[pl.ds(0, hidden), pl.ds(place, length)],
            r.load_sem.at[small + 2],
        )
        for columns, place, length in result_columns(c)
    ]

    barrier = pltpu.get_barrier_semaphore()
    for step in range(1, 2 * LINE):
        pl.semaphore_signal(
            barrier, inc=1, device_id=((e + step) % (2 * LINE), t), device_id_type=MESH
        )
    for other in (sibling, partner):
        pl.semaphore_signal(barrier, inc=1, device_id=other, device_id_type=MESH)

    for load in loads[:4]:
        load.wait()
    for load in loads[small:] + down_loads:
        load.start()
    widened = r.token[...].astype(jnp.float32)
    scale = lax.rsqrt(jnp.mean(widened * widened, axis=-1, keepdims=True) + EPS)
    r.own[...] = (widened * scale * r.gain[...]).astype(jnp.bfloat16)

    expert = lax.broadcasted_iota(jnp.int32, (2 * LINE, tokens), 0)
    named = jnp.zeros((2 * LINE, tokens), jnp.float32)
    for k in range(TOPK):
        named = named + jnp.where(expert == r.routing[k : k + 1], r.route_weight[k : k + 1], 0.0)
    r.shares[e] = named

    ahead = (
        lax.broadcasted_iota(jnp.int32, (tokens, tokens), 0)
        <= lax.broadcasted_iota(jnp.int32, (tokens, tokens), 1)
    ).astype(jnp.float32)
    slot = (lax.broadcasted_iota(jnp.int32, (SLOTS, tokens), 0) + 1).astype(jnp.float32)

    def ranked(block):
        routed = jnp.where(r.shares[block] > 0.0, 1.0, 0.0)
        r.ranks[block] = jnp.dot(routed, ahead, preferred_element_type=jnp.float32)

    def one_hot(block, expert):
        weight = r.shares[block, pl.ds(expert, 1), :]
        here = (r.ranks[block, pl.ds(expert, 1), :] == slot) & (weight > 0.0)
        return jnp.where(here, 1.0, 0.0), jnp.sum(jnp.where(here, weight, 0.0), axis=1, keepdims=True)

    def keep_weight(at, half, found):
        r.slot_weight[at, half * SLOTS : (half + 1) * SLOTS, :] = jnp.broadcast_to(found, (SLOTS, 128))

    def prepare(at):
        ranked(at * 2 + x)
        hot, found = one_hot(at * 2 + x, e)
        keep_weight(at, 0, found)
        r.hot[at, 0:SLOTS, :] = hot.astype(jnp.bfloat16)
        r.hot[at, SLOTS : 2 * SLOTS, :] = one_hot(at * 2 + x, z * 2 + 1 - x)[0].astype(jnp.bfloat16)

    def prepare_other(at):
        ranked(at * 2 + 1 - x)
        keep_weight(at, 1, one_hot(at * 2 + 1 - x, e)[1])

    prepare(z)
    for load in loads[4:small]:
        load.wait()
    pl.semaphore_wait(barrier, 2 * LINE + 1)

    parts = parts_of(lone, both)
    start_of_both = 2 * lone + c * both
    own_columns = (
        sections[0][0], aligned(start_of_both, both // 2), aligned(start_of_both + both // 2, both // 2)
    )

    def rows_of(half):
        return pl.ds(half * SLOTS, SLOTS)

    def own_along(up, part):
        start, length = parts[part]
        return copy(
            r.own.at[:, own_columns[part]], r.dense.at[z, :, pl.ds(start, length)],
            r.own_send.at[up], r.along_recv.at[z, part], (e + 4 * up - 2, t),
        )

    def onward(at, part):
        start, length = parts[part]
        view = r.dense.at[at, :, pl.ds(start, length)]
        to = (jnp.where(at < z, e + 2, e - 2), t)
        return copy(view, view, r.onward_send.at[at], r.along_recv.at[at, part], to)

    def across(at, part):
        start, length = parts[part]
        return copy(
            r.aside.at[at, :, pl.ds(start, length)],
            r.packed.at[at, rows_of(1), pl.ds(start, length)],
            r.across_send.at[at], r.across_recv.at[at, part], beside,
        )

    def to_partner(at, half):
        return copy(
            r.packed.at[at, rows_of(half), pl.ds(0, lone)],
            r.packed.at[at, rows_of(half), pl.ds(2 * held, lone)],
            r.partner_send.at[at], r.partner_recv.at[at, half], partner,
        )

    core_parts = [(start, held + start, length) for start, length in parts]
    core_parts.append((2 * held, 2 * held + lone, lone))

    def to_sibling(at, half, kind):
        start, landing, length = core_parts[kind]
        return copy(
            r.packed.at[at, rows_of(half), pl.ds(start, length)],
            r.packed.at[at, rows_of(half), pl.ds(landing, length)],
            r.core_send.at[at], r.core_recv.at[at], sibling,
        )

    def share_copy(step):
        to = (e + step) % (2 * LINE)
        return copy(r.shares.at[e], r.shares.at[e], r.share_send, r.share_recv.at[e], (to, t))

    def share_in(block):
        return copy(
            r.shares.at[block], r.shares.at[block], r.share_send, r.share_recv.at[block], beside
        )

    def own_along_start(part):
        @pl.when(z < LINE - 1)
        def _():
            own_along(1, part).start()

        @pl.when(z > 0)
        def _():
            own_along(0, part).start()

    def pack_aside(part):
        start, length = parts[part]
        found = jnp.dot(
            r.hot[z, SLOTS : 2 * SLOTS, :], r.own[:, own_columns[part]],
            preferred_element_type=jnp.float32,
        )
        r.aside[z, :, start : start + length] = found.astype(jnp.bfloat16)
        across(z, part).start()

    queries = r.query_hbm.shape[0]

    def halo_copy(which):
        src = (r.key, r.value)[which].at[pl.ds(queries - WINDOW_KEYS, WINDOW_KEYS)]
        to = ((e + 1) % (2 * LINE), t)
        return copy(src, r.halo.at[which], r.halo_send, r.halo_recv.at[which], to)

    @pl.when(e < 2 * LINE - 1)
    def _():
        halo_copy(0).start()
        halo_copy(1).start()

    @pl.when(e == 0)
    def _():
        r.halo[...] = jnp.zeros_like(r.halo)

    own_along_start(0)
    for step in range(1, 2 * LINE):
        share_copy(step).start()
    pack_aside(0)
    for part in range(1, len(parts)):
        own_along_start(part)
        pack_aside(part)

    def down_copy(number):
        columns, place, length = result_columns(1 - c)[number]
        return copy(
            r.down_hbm.at[:, columns], r.down.at[pl.ds(hidden, hidden), pl.ds(place, length)],
            r.down_send, r.down_recv, sibling,
        )

    for number in range(3):
        down_copy(number).start()

    for columns, place, length in sections:
        found = jnp.dot(r.hot[z, 0:SLOTS, :], r.own[:, columns], preferred_element_type=jnp.float32)
        r.packed[z, 0:SLOTS, place : place + length] = found.astype(jnp.bfloat16)

    kv_heads = r.key_hbm.shape[1] // HEAD_SIZE
    group = r.query_hbm.shape[1] // HEAD_SIZE // kv_heads
    span = queries // 4
    here = lax.broadcasted_iota(jnp.int32, (WINDOW_KEYS, 2 * WINDOW_KEYS), 0)
    there = lax.broadcasted_iota(jnp.int32, (WINDOW_KEYS, 2 * WINDOW_KEYS), 1)

    def attend(number, kv):
        begin = number * WINDOW_KEYS
        permitted = (there > here) & (there <= here + WINDOW_KEYS)
        if number == 0:
            permitted = permitted & ((there >= WINDOW_KEYS) | (e > 0))
        lanes = slice(kv * HEAD_SIZE, (kv + 1) * HEAD_SIZE)
        if number == 0:
            keys = jnp.concatenate([r.halo[0][:, lanes], r.key[0:WINDOW_KEYS, lanes]], axis=0)
            values = jnp.concatenate([r.halo[1][:, lanes], r.value[0:WINDOW_KEYS, lanes]], axis=0)
        else:
            keys = r.key[begin - WINDOW_KEYS : begin + WINDOW_KEYS, lanes]
            values = r.value[begin - WINDOW_KEYS : begin + WINDOW_KEYS, lanes]
        for member in range(group):
            head = kv * group + member
            columns = slice(head * HEAD_SIZE, (head + 1) * HEAD_SIZE)
            scores = lax.dot_general(
                r.query[begin : begin + WINDOW_KEYS, columns],
                keys,
                (((1,), (1,)), ((), ())),
                preferred_element_type=jnp.float32,
            ) * HEAD_SIZE ** (-0.5)
            scores = jnp.where(permitted, scores, -jnp.inf)
            sink = r.sink[head]
            highest = jnp.maximum(jnp.max(scores, axis=-1, keepdims=True), sink)
            numerator = jnp.exp(scores - highest)
            denominator = jnp.sum(numerator, axis=-1, keepdims=True) + jnp.exp(sink - highest)
            weights = (numerator / denominator).astype(jnp.bfloat16)
            found = jnp.dot(weights, values, preferred_element_type=jnp.float32)
            r.attended[begin : begin + WINDOW_KEYS, columns] = found.astype(jnp.bfloat16)

    def halo_wait():
        @pl.when(e > 0)
        def _():
            halo_copy(0).wait_recv()
            halo_copy(1).wait_recv()

    def mixed_core(half):
        at = pl.multiple_of((half * 2 + 1 - c) * span, 16)
        return copy(
            r.mixed.at[pl.ds(at, span)], r.mixed_core.at[half],
            r.mixed_core_send, r.mixed_core_recv.at[half], sibling,
        )

    cut = span // MIXED_CUTS

    def mixed_pair(number):
        at = pl.multiple_of(((1 - y) * 2 + c) * span + number * cut, 16)
        return copy(
            r.mixed.at[pl.ds(at, cut)], r.mixed_pair.at[pl.ds(number * cut, cut)],
            r.mixed_pair_send, r.mixed_pair_recv.at[number], partner,
        )

    def mixed_rows(half):
        return pl.ds(pl.multiple_of((half * 2 + c) * span, 16), span)

    def mix():
        loads[small].wait()
        for place in range(0, width, quarter):
            columns = slice(place, place + quarter)
            r.mixed[:, columns] = jnp.dot(
                r.attended[...], r.project[:, columns], preferred_element_type=jnp.float32
            ).astype(jnp.bfloat16)
        for half in range(2):
            mixed_core(half).start()

    def mix_onward():
        for half in range(2):
            mixed_core(half).wait_recv()
            total = r.mixed[mixed_rows(half), :].astype(jnp.float32)
            r.mixed[mixed_rows(half), :] = (
                total + r.mixed_core[half].astype(jnp.float32)
            ).astype(jnp.bfloat16)

    def forward(k, part):
        onward(near[k], part).wait_recv()
        onward(near[k], part).start()

    def forward_middle(k, part):
        @pl.when(at_middle)
        def _():
            forward(k, part)

    def wait_end(k, part):
        @pl.when(at_end)
        def _():
            onward(near[k], part).wait_recv()

    def pack(k, part):
        at = near[k]
        start, length = parts[part]
        found = jnp.dot(
            r.hot[at], r.dense[at, :, start : start + length], preferred_element_type=jnp.float32
        ).astype(jnp.bfloat16)
        r.aside[at, :, start : start + length] = found[SLOTS : 2 * SLOTS]
        across(at, part).start()
        r.packed[at, 0:SLOTS, start : start + length] = found[0:SLOTS]
        if part == 0:
            to_partner(at, 0).start()
        to_sibling(at, 0, part).start()

    def take_across(k, part):
        at = near[k]
        across(at, part).wait_recv()
        if part == 0:
            to_partner(at, 1).start()
        to_sibling(at, 1, part).start()

    def take_partner(k, half):
        to_partner(near[k], half).wait_recv()
        to_sibling(near[k], half, len(parts)).start()

    def get_ready(k):
        share_in(near[k] * 2 + x).wait_recv()
        prepare(near[k])

    def get_other_ready(k):
        share_in(near[k] * 2 + 1 - x).wait_recv()
        prepare_other(near[k])

    def active_copy(at):
        return copy(
            r.active.at[at, :, pl.ds(0, hidden)], r.active.at[at, :, pl.ds(hidden, hidden)],
            r.active_send.at[at], r.active_recv.at[at], sibling,
        )

    def enter(k):
        at = near[k]
        rows = pl.ds(0, 2 * SLOTS) if k else pl.ds(0, SLOTS)
        arrived = r.packed.at[at, rows, pl.ds(0, held + lone)]
        copy(arrived, arrived, r.core_send.at[at], r.core_recv.at[at], sibling).wait_recv()
        pre = jnp.dot(r.packed[at], r.both_weights[...], preferred_element_type=jnp.float32)
        gate_cut = jnp.minimum(pre[:, 0:hidden], CLAMP)
        up_pre = pre[:, hidden : 2 * hidden]
        r.active[at, :, 0:hidden] = (
            (jnp.clip(up_pre, -CLAMP, CLAMP) + 1.0) * gate_cut * jax.nn.sigmoid(SLOPE * gate_cut)
        ).astype(jnp.bfloat16)
        active_copy(at).start()

    late = quarter - early
    chunks = chunks_of(quarter, early)

    def pair_copy(at, half):
        return copy(
            r.results.at[at, rows_of(half), pl.ds(carried, early)], r.pair.at[at, rows_of(half), :],
            r.pair_send.at[at], r.pair_recv.at[at, half], partner,
        )

    def side_copy(at, chunk):
        start, length = chunks[chunk]
        return copy(
            r.results.at[at, rows_of(1), pl.ds(start, length)], r.side.at[at, :, pl.ds(start, length)],
            r.side_send.at[at], r.side_recv.at[at, chunk], beside,
        )

    def leave(k):
        at = near[k]
        active_copy(at).wait_recv()

        def finish(start, length):
            found = jnp.dot(
                r.active[at], r.down[:, start : start + length], preferred_element_type=jnp.float32
            )
            r.results[at, :, start : start + length] = (found * r.slot_weight[at][:, 0:1]).astype(
                jnp.bfloat16
            )

        finish(carried, early)
        if k > 1:
            send_pair(k, 1)
            send_pair(k, 0)
        for chunk in range(2):
            finish(*chunks[chunk])
            if k:
                side_copy(at, chunk).start()
        finish(0, early)

    def send_pair(k, half):
        pair_copy(near[k], half).start()

    def send_side(k):
        side_copy(near[k], 0).start()
        side_copy(near[k], 1).start()

    def take_pair(k, half):
        at = near[k]
        pair_copy(at, half).wait_recv()
        rows = slice(half * SLOTS, (half + 1) * SLOTS)
        for chunk in range(2, len(chunks)):
            columns = slice(chunks[chunk][0], chunks[chunk][0] + chunks[chunk][1])
            total = r.results[at, rows, columns].astype(jnp.float32)
            r.results[at, rows, columns] = (
                total + r.pair[at, rows, columns].astype(jnp.float32)
            ).astype(jnp.bfloat16)
            if half:
                side_copy(at, chunk).start()

    def line_copy(way, at, chunk):
        start, length = chunks[chunk]
        to = (jnp.where(at > z, e + 2, e - 2), t)
        return copy(
            r.line_out.at[at, :, pl.ds(start, length)], r.line_in.at[way, at, :, pl.ds(start, length)],
            r.line_send.at[at], r.line_recv.at[way, at, chunk], to,
        )

    last = copy(r.line_out.at[z, :, pl.ds(quarter, late)], r.last, r.last_send, r.last_recv, partner)

    def line_step(k, chunk, middle):
        at = near[k]
        start, length = chunks[chunk]
        columns = slice(start, start + length)
        side_copy(at, chunk).wait_recv()
        both_sides = jnp.concatenate([r.results[at, 0:SLOTS, columns], r.side[at, :, columns]], axis=0)
        total = lax.dot_general(
            r.hot[at], both_sides, (((0,), (0,)), ((), ())), preferred_element_type=jnp.float32
        )
        if k:
            way = jnp.where(at > z, 0, 1)
            ways = (way,) if middle else ()
        elif middle:
            ways = (0, 1)
        else:
            ways = (jnp.where(z == 0, 1, 0),)
        for way in ways:
            line_copy(way, at, chunk).wait_recv()
            total = total + r.line_in[way, at, :, columns].astype(jnp.float32)
        if k or chunk == 0:
            r.line_out[at, :, columns] = total.astype(jnp.bfloat16)
            if k:
                line_copy(way, at, chunk).start()
            else:
                last.start()
        elif chunk == 1:
            r.final[...] = total
        else:
            r.out[:, columns] = total.astype(jnp.bfloat16)

    def arrive(k, part):
        wait_end(k, part)
        if k == 1:
            forward_middle(1, part)
        if k < LINE - 1:
            forward_middle(k + 1, part)

    def end_packs(k, part):
        at_places(at_end, (pack, k, part))

    def middle_packs(k, part):
        at_places(at_middle, (pack, k, part))

    def send_mixed(number):
        mixed_pair(number).start()

    def finish_mixed():
        for number in range(MIXED_CUTS):
            mixed_pair(number).wait_recv()
        total = r.mixed[mixed_rows(y), :].astype(jnp.float32)
        r.mixer[...] = (total + r.mixed_pair[...].astype(jnp.float32)).astype(jnp.bfloat16)

    def at_places(which, *steps):
        @pl.when(which)
        def _():
            for step in steps:
                step[0](*step[1:])

    def end_lines(k, *which):
        at_places(at_end, *[(line_step, k, chunk, False) for chunk in which])

    def middle_lines(k, *which):
        at_places(at_middle, *[(line_step, k, chunk, True) for chunk in which])

    def sent(view, semaphore):
        copy(view, view, semaphore, semaphore, sibling).wait_send()

    def drain_dispatch():
        @pl.when(z < LINE - 1)
        def _():
            sent(r.dense.at[0], r.own_send.at[1])

        @pl.when(z > 0)
        def _():
            sent(r.dense.at[0], r.own_send.at[0])

        @pl.when(at_middle)
        def _():
            for k in range(1, LINE):
                sent(r.dense.at[near[k]], r.onward_send.at[near[k]])

        @pl.when(e < 2 * LINE - 1)
        def _():
            sent(r.halo, r.halo_send)

        sent(r.shares.at[pl.ds(0, 2 * LINE - 1)], r.share_send)
        sent(r.down.at[pl.ds(0, hidden)], r.down_send)
        sent(r.mixed_core, r.mixed_core_send)
        for k in range(LINE):
            at = near[k]
            sent(r.aside.at[at], r.across_send.at[at])
            rows = pl.ds(0, 2 * SLOTS) if k else pl.ds(0, SLOTS)
            sent(r.packed.at[at, rows, pl.ds(0, lone)], r.partner_send.at[at])
            sent(r.packed.at[at, rows, pl.ds(0, held + lone)], r.core_send.at[at])
            active_copy(at).wait_send()

    def drain_return():
        sent(r.mixed_pair, r.mixed_pair_send)
        for at in range(LINE):
            sent(r.pair.at[at], r.pair_send.at[at])
            sent(r.side.at[at], r.side_send.at[at])

    attend(1, 0)
    attend(1, 1)
    take_across(0, 0)
    get_other_ready(0)
    get_ready(1)
    arrive(1, 0)
    pack(1, 0)
    halo_wait()
    attend(0, 0)
    attend(0, 1)
    take_across(0, 1)
    mix()
    arrive(1, 1)
    pack(1, 1)
    take_partner(0, 1)
    take_across(0, 2)
    mix_onward()
    arrive(1, 2)
    pack(1, 2)
    get_ready(2)
    middle_packs(2, 0)
    middle_packs(2, 1)
    middle_packs(2, 2)
    take_across(1, 0)
    send_mixed(0)
    get_other_ready(1)
    pltpu.make_async_copy(r.both_weights, r.both_weights, r.load_sem.at[small + 1]).wait()
    arrived = r.down.at[pl.ds(0, hidden)]
    pltpu.make_async_copy(arrived, arrived, r.load_sem.at[small + 2]).wait()
    copy(arrived, arrived, r.down_send, r.down_recv, sibling).wait_recv()
    enter(0)
    take_partner(1, 0)
    take_across(1, 1)
    arrive(2, 0)
    end_packs(2, 0)
    get_ready(3)
    middle_packs(3, 0)
    leave(0)
    take_across(1, 2)
    take_partner(1, 1)
    arrive(2, 1)
    end_packs(2, 1)
    middle_packs(3, 1)
    take_across(2, 0)
    send_mixed(1)
    enter(1)
    arrive(2, 2)
    end_packs(2, 2)
    middle_packs(3, 2)
    take_across(2, 1)
    take_partner(2, 0)
    leave(1)
    get_other_ready(2)
    arrive(3, 0)
    end_packs(3, 0)
    send_pair(1, 1)
    take_across(2, 2)
    take_partner(2, 1)
    arrive(3, 1)
    end_packs(3, 1)
    enter(2)
    take_across(3, 0)
    send_pair(1, 0)
    arrive(3, 2)
    end_packs(3, 2)
    end_lines(1, 0, 1)
    leave(2)
    take_across(3, 1)
    take_pair(1, 1)
    take_partner(3, 0)
    take_across(3, 2)
    take_pair(1, 0)
    take_partner(3, 1)
    get_other_ready(3)
    end_lines(2, 0, 1)
    enter(3)
    end_lines(1, 2, 3)
    take_pair(2, 1)
    leave(3)
    send_pair(0, 1)
    send_pair(0, 0)
    send_mixed(2)
    send_mixed(3)
    take_pair(2, 0)
    middle_lines(1, 0, 1)
    end_lines(2, 2, 3)
    take_pair(3, 1)
    send_side(0)
    end_lines(3, 0, 1)
    take_pair(3, 0)
    middle_lines(1, 2, 3)
    middle_lines(3, 0, 1)
    end_lines(3, 2, 3)
    middle_lines(2, 0)
    middle_lines(3, 2)
    middle_lines(2, 1)
    middle_lines(3, 3)
    take_pair(0, 1)
    take_pair(0, 0)
    drain_dispatch()
    middle_lines(2, 2, 3)
    middle_lines(0, 0, 1)
    end_lines(0, 0, 1)
    finish_mixed()
    middle_lines(0, 2, 3)
    end_lines(0, 2)
    drain_return()
    end_lines(0, 3)

    last.wait_recv()
    r.out[:, early:quarter] = (r.final[...] + r.last[...].astype(jnp.float32)).astype(
        jnp.bfloat16
    )
    last.wait_send()
    for k in range(1, LINE):
        sent(r.line_out.at[near[k]], r.line_send.at[near[k]])


def layer_call(
    rows, gain, routing, route_weight, queries, keys, values, sinks, project, gate_one, up_one, down_one
):
    tokens, width = rows.shape
    quarter, lone, both, early, carried = sizes_of(width)
    parts, chunks = len(parts_of(lone, both)), len(chunks_of(quarter, early))
    blocks = 2 * LINE
    hidden = gate_one.shape[1]
    kept = jnp.bfloat16
    dma = pltpu.SemaphoreType.DMA
    span = queries.shape[0] // 4
    stays = pl.BlockSpec(memory_space=pl.ANY)
    in_vmem = pl.BlockSpec(memory_space=pltpu.VMEM)
    scratch = dict(
        token=pltpu.VMEM(rows.shape, kept),
        gain=pltpu.VMEM(gain.shape, jnp.float32),
        routing=pltpu.VMEM(routing.shape, jnp.int32),
        route_weight=pltpu.VMEM(route_weight.shape, jnp.float32),
        query=pltpu.VMEM(queries.shape, kept),
        key=pltpu.VMEM(keys.shape, kept),
        value=pltpu.VMEM(values.shape, kept),
        sink=pltpu.SMEM(sinks.shape, jnp.float32),
        own=pltpu.VMEM((tokens, width), kept),
        dense=pltpu.VMEM((LINE, tokens, lone + both), kept),
        packed=pltpu.VMEM((LINE, 2 * SLOTS, width), kept),
        aside=pltpu.VMEM((LINE, SLOTS, lone + both), kept),
        both_weights=pltpu.VMEM((width, 2 * hidden), kept),
        down=pltpu.VMEM((2 * hidden, 2 * quarter), kept),
        project=pltpu.VMEM(project.shape, kept),
        halo=pltpu.VMEM((2, WINDOW_KEYS, keys.shape[1]), kept),
        attended=pltpu.VMEM(queries.shape, kept),
        mixed=pltpu.VMEM((queries.shape[0], width), kept),
        mixed_core=pltpu.VMEM((2, span, width), kept),
        mixed_pair=pltpu.VMEM((span, width), kept),
        shares=pltpu.VMEM((blocks, 8, tokens), jnp.float32),
        ranks=pltpu.VMEM((blocks, 8, tokens), jnp.float32),
        hot=pltpu.VMEM((LINE, 2 * SLOTS, tokens), kept),
        slot_weight=pltpu.VMEM((LINE, 2 * SLOTS, 128), jnp.float32),
        active=pltpu.VMEM((LINE, 2 * SLOTS, 2 * hidden), kept),
        results=pltpu.VMEM((LINE, 2 * SLOTS, 2 * quarter), kept),
        pair=pltpu.VMEM((LINE, 2 * SLOTS, early), kept),
        side=pltpu.VMEM((LINE, SLOTS, carried), kept),
        line_out=pltpu.VMEM((LINE, tokens, carried), kept),
        line_in=pltpu.VMEM((2, LINE, tokens, carried), kept),
        last=pltpu.VMEM((tokens, quarter - early), kept),
        final=pltpu.VMEM((tokens, quarter - early), jnp.float32),
        load_sem=dma((11,)),
        halo_send=dma,
        halo_recv=dma((2,)),
        mixed_core_send=dma,
        mixed_core_recv=dma((2,)),
        mixed_pair_send=dma,
        mixed_pair_recv=dma((MIXED_CUTS,)),
        share_send=dma,
        share_recv=dma((blocks,)),
        own_send=dma((2,)),
        onward_send=dma((LINE,)),
        along_recv=dma((LINE, parts)),
        across_send=dma((LINE,)),
        across_recv=dma((LINE, parts)),
        partner_send=dma((LINE,)),
        partner_recv=dma((LINE, 2)),
        core_send=dma((LINE,)),
        core_recv=dma((LINE,)),
        down_send=dma,
        down_recv=dma,
        active_send=dma((LINE,)),
        active_recv=dma((LINE,)),
        pair_send=dma((LINE,)),
        pair_recv=dma((LINE, 2)),
        side_send=dma((LINE,)),
        side_recv=dma((LINE, chunks)),
        line_send=dma((LINE,)),
        line_recv=dma((2, LINE, chunks)),
        last_send=dma,
        last_recv=dma,
    )
    return pl.pallas_call(
        layer_kernel,
        out_shape=(
            pltpu.VMEM((span, width), kept),
            pltpu.VMEM((tokens, quarter), kept),
        ),
        in_specs=[stays] * 12,
        out_specs=(in_vmem, in_vmem),
        scratch_shapes=[scratch[name] for name in NAMES[14:]],
        compiler_params=pltpu.CompilerParams(
            collective_id=0, has_side_effects=True, vmem_limit_bytes=60 * 1024 * 1024
        ),
        cost_estimate=pl.CostEstimate(
            flops=8 * blocks * tokens * width * hidden,
            bytes_accessed=8 * width * hidden,
            transcendentals=0,
        ),
    )(rows, gain, routing, route_weight, queries, keys, values, sinks, project, gate_one, up_one, down_one)


def shards(
    projected_queries,
    key_proj,
    projected_values,
    head_sink_logits,
    out_weight,
    expert_input,
    norm_gain,
    routing,
    route_weight,
    gate_weight,
    up_weight,
    down_weight,
):
    token_rows = expert_input.shape[0]
    experts = lax.axis_size("ep")
    capacity = max(3 * token_rows * TOPK // (2 * experts), 2)
    col_share = D // lax.axis_size("tp")
    if (experts, lax.axis_size("tp")) == (2 * LINE, 4) and token_rows == 128:
        return layer_call(
            expert_input,
            norm_gain[None, :],
            routing.T,
            route_weight.T,
            projected_queries,
            key_proj,
            projected_values,
            head_sink_logits,
            out_weight,
            gate_weight[0],
            up_weight[0],
            down_weight[0],
        )
    widened = expert_input.astype(jnp.float32)
    normed = (
        widened
        * lax.rsqrt(jnp.mean(widened * widened, axis=-1, keepdims=True) + EPS)
        * norm_gain[None, :]
    ).astype(jnp.bfloat16)
    query_rows = projected_queries.shape[0]
    kv_heads = key_proj.shape[1] // HEAD_SIZE
    heads_per_group = projected_queries.shape[1] // HEAD_SIZE // kv_heads
    count_of_blocks = query_rows // WINDOW_KEYS
    prior_key, prior_value = passed_along(
        (key_proj[query_rows - WINDOW_KEYS :], projected_values[query_rows - WINDOW_KEYS :]),
        "ep",
        1,
    )
    key_all = jnp.concatenate([prior_key, key_proj], axis=0)
    value_all = jnp.concatenate([prior_value, projected_values], axis=0)
    window_keys = jnp.concatenate(
        [
            key_all[:-WINDOW_KEYS].reshape(count_of_blocks, WINDOW_KEYS, kv_heads, HEAD_SIZE),
            key_all[WINDOW_KEYS:].reshape(count_of_blocks, WINDOW_KEYS, kv_heads, HEAD_SIZE),
        ],
        axis=1,
    )
    window_values = jnp.concatenate(
        [
            value_all[:-WINDOW_KEYS].reshape(count_of_blocks, WINDOW_KEYS, kv_heads, HEAD_SIZE),
            value_all[WINDOW_KEYS:].reshape(count_of_blocks, WINDOW_KEYS, kv_heads, HEAD_SIZE),
        ],
        axis=1,
    )
    query_blocks = projected_queries.reshape(
        count_of_blocks, WINDOW_KEYS, kv_heads, heads_per_group, HEAD_SIZE
    )
    scores = jnp.einsum(
        "nqhgd,nshd->nhgqs", query_blocks, window_keys, preferred_element_type=jnp.float32
    ) * HEAD_SIZE ** (-0.5)
    offset = lax.axis_index("ep") * query_rows
    block_ids = jnp.arange(count_of_blocks)[:, None, None] * WINDOW_KEYS + offset
    query_pos = block_ids + jnp.arange(WINDOW_KEYS)[None, :, None]
    key_pos = block_ids - WINDOW_KEYS + jnp.arange(2 * WINDOW_KEYS)[None, None, :]
    permitted_mask = (key_pos <= query_pos) & (query_pos - key_pos < WINDOW_KEYS) & (key_pos >= 0)
    scores = jnp.where(permitted_mask[:, None, None, :, :], scores, -jnp.inf)
    sink_col = head_sink_logits.reshape(kv_heads, heads_per_group)[None, :, :, None, None]
    highest = jnp.maximum(jnp.max(scores, axis=-1, keepdims=True), sink_col)
    numerator = jnp.exp(scores - highest)
    denominator = jnp.sum(numerator, axis=-1, keepdims=True) + jnp.exp(sink_col - highest)
    weights = (numerator / denominator).astype(jnp.bfloat16)
    attended = jnp.einsum(
        "nhgqs,nshd->nqhgd", weights, window_values, preferred_element_type=jnp.float32
    )
    attended = attended.astype(jnp.bfloat16).reshape(
        query_rows, kv_heads * heads_per_group * HEAD_SIZE
    )
    mixer_output = lax.psum_scatter(
        jnp.dot(attended, out_weight, preferred_element_type=jnp.float32).astype(jnp.bfloat16),
        "tp",
        scatter_dimension=0,
        tiled=True,
    )
    flat_ids = routing.reshape(-1)
    onehot = (flat_ids[:, None] == jnp.arange(experts, dtype=jnp.int32)[None, :]).astype(jnp.int32)
    rank_in = jnp.cumsum(onehot, axis=0) - 1
    target = flat_ids * capacity + jnp.sum(rank_in * onehot, axis=1)
    tok_ids = jnp.arange(token_rows * TOPK) // TOPK
    slot_tok = jnp.full((experts * capacity,), token_rows, jnp.int32).at[target].set(tok_ids)
    gate_one = gate_weight[0]
    up_one = up_weight[0]
    own_cols = lax.dynamic_slice_in_dim(normed, lax.axis_index("tp") * col_share, col_share, 1)
    extended = jnp.concatenate([own_cols, jnp.zeros((1, col_share), jnp.bfloat16)], axis=0)
    outgoing = jnp.take(extended, slot_tok, axis=0).reshape(experts, capacity, col_share)
    arrived = lax.all_to_all(outgoing, "ep", split_axis=0, concat_axis=0, tiled=True).reshape(
        experts * capacity, col_share
    )
    portion = lax.all_gather(arrived, "tp", axis=1, tiled=True)
    gate_pre = jnp.dot(portion, gate_one, preferred_element_type=jnp.float32)
    up_pre = jnp.dot(portion, up_one, preferred_element_type=jnp.float32)
    gate_cut = jnp.minimum(gate_pre, CLAMP)
    activated = (
        (jnp.clip(up_pre, -CLAMP, CLAMP) + 1.0) * gate_cut * jax.nn.sigmoid(SLOPE * gate_cut)
    ).astype(jnp.bfloat16)
    partial_value = jnp.dot(activated, down_weight[0], preferred_element_type=jnp.float32)
    expert_result = lax.psum_scatter(
        partial_value.astype(jnp.bfloat16), "tp", scatter_dimension=1, tiled=True
    )
    returned = lax.all_to_all(
        expert_result.reshape(experts, capacity, col_share),
        "ep",
        split_axis=0,
        concat_axis=0,
        tiled=True,
    )
    picked = jnp.take(returned.reshape(experts * capacity, col_share), target, axis=0)
    picked = picked.astype(jnp.float32).reshape(token_rows, TOPK, col_share)
    expert_output = jnp.sum(picked * route_weight[:, :, None], axis=1).astype(jnp.bfloat16)
    return (mixer_output, expert_output)


def solution(mesh):
    placed = (
        P("ep", "tp"),
        P("ep", "tp"),
        P("ep", "tp"),
        P("tp"),
        P("tp", None),
        P("ep", None),
        P(),
        P("ep", None),
        P("ep", None),
        P("ep", None, "tp"),
        P("ep", None, "tp"),
        P("ep", "tp", None),
    )
    return jax.shard_map(
        shards,
        mesh=mesh,
        in_specs=placed,
        out_specs=(P(("ep", "tp"), None), P("ep", "tp")),
        check_vma=False,
    )
```

```python
import types

import jax
import jax.numpy as jnp
from jax import lax
from jax.experimental import pallas as pl
from jax.experimental.pallas import tpu as pltpu
from jax.sharding import PartitionSpec as P

D = 4096
HEAD_SIZE = 64
WINDOW_KEYS = 128
TOPK = 4


EPS = 1e-06
CLAMP = 7.0
SLOPE = 1.702


def passed_along(block, axis, distance):
    devices = range(lax.axis_size(axis))
    route = [(i - distance, i) for i in devices if i - distance in devices]
    return lax.ppermute(block, axis, route)


LINE = 4
SLOTS = 96
LONE = 4
EARLY = 5
MIXED_CUTS = 4
MESH = pl.DeviceIdType.MESH

NAMES = (
    "token_hbm", "gain_hbm", "routing_hbm", "route_weight_hbm", "query_hbm", "key_hbm",
    "value_hbm", "sink_hbm", "project_hbm", "gate_hbm", "up_hbm", "down_hbm", "mixer", "out",
    "token", "gain", "routing", "route_weight", "query", "key", "value", "sink", "own", "dense",
    "packed", "aside", "both_weights", "down", "project", "halo", "attended", "mixed",
    "mixed_core", "mixed_pair", "shares", "ranks", "hot", "slot_weight", "active", "results",
    "pair", "side", "line_out", "line_in", "last", "final", "load_sem", "halo_send", "halo_recv",
    "mixed_core_send", "mixed_core_recv", "mixed_pair_send", "mixed_pair_recv", "share_send",
    "share_recv", "own_send", "onward_send", "along_recv", "across_send", "across_recv",
    "partner_send", "partner_recv", "core_send", "core_recv", "down_send", "down_recv",
    "active_send", "active_recv", "pair_send", "pair_recv", "side_send", "side_recv", "line_send",
    "line_recv", "last_send", "last_recv",
)


def chosen(z, values):
    result = jnp.int32(values[0])
    for place in range(1, LINE):
        result = jnp.where(z == place, jnp.int32(values[place]), result)
    return result


def nearest_first(place):
    return sorted(range(LINE), key=lambda other: (abs(other - place), abs(2 * other - LINE + 1)))


def sizes_of(width):
    quarter = width // 4
    lone = width * LONE // 32
    both = (width - 4 * lone) // 2
    early = width * EARLY // 32
    return quarter, lone, both, early, 2 * quarter - early


def parts_of(lone, both):
    return (0, lone), (lone, both // 2), (lone + both // 2, both // 2)


def chunks_of(quarter, early):
    late, first = quarter - early, (early + 128) // 256 * 128
    return (quarter, late), (early, late), (0, first), (first, early - first)


def layer_kernel(*refs):
    r = types.SimpleNamespace(**dict(zip(NAMES, refs)))
    e, t = lax.axis_index("ep"), lax.axis_index("tp")
    z, x, y, c = e // 2, e % 2, t // 2, t % 2
    tokens, width = r.token_hbm.shape
    quarter, lone, both, early, carried = sizes_of(width)
    held = lone + both
    hidden = r.gate_hbm.shape[1]
    sibling, partner, beside = (e, y * 2 + 1 - c), (e, (1 - y) * 2 + c), (z * 2 + 1 - x, t)
    at_end = (z == 0) | (z == LINE - 1)
    at_middle = (z > 0) & (z < LINE - 1)
    near = [chosen(z, [nearest_first(place)[j] for place in range(LINE)]) for j in range(LINE)]

    def copy(src, dst, send, recv, to):
        return pltpu.make_async_remote_copy(
            src_ref=src, dst_ref=dst, send_sem=send, recv_sem=recv, device_id=to, device_id_type=MESH
        )

    def aligned(start, length):
        return pl.ds(pl.multiple_of(start, 128), length)

    def lone_of(row, core):
        return aligned(row * (width - 2 * lone) + core * lone, lone)

    def both_of(core):
        return aligned(2 * lone + core * both, both)

    sections = [
        (lone_of(y, c), 0, lone),
        (both_of(c), lone, both),
        (lone_of(y, 1 - c), held, lone),
        (both_of(1 - c), held + lone, both),
        (lone_of(1 - y, c), 2 * held, lone),
        (lone_of(1 - y, 1 - c), 2 * held + lone, lone),
    ]
    mine, theirs = (y * 2 + c) * quarter, ((1 - y) * 2 + c) * quarter

    def result_columns(core):
        own, other = (y * 2 + core) * quarter, ((1 - y) * 2 + core) * quarter
        return [
            (aligned(own, quarter), 0, quarter),
            (aligned(other + early, quarter - early), quarter, quarter - early),
            (aligned(other, early), carried, early),
        ]

    pieces = [
        (r.routing_hbm, r.routing), (r.route_weight_hbm, r.route_weight), (r.token_hbm, r.token),
        (r.gain_hbm, r.gain), (r.sink_hbm, r.sink), (r.query_hbm, r.query), (r.key_hbm, r.key),
        (r.value_hbm, r.value), (r.project_hbm, r.project),
    ]
    small = len(pieces) - 1
    for columns, place, length in sections:
        for number, weights in enumerate((r.gate_hbm, r.up_hbm)):
            pieces.append(
                (
                    weights.at[columns, :],
                    r.both_weights.at[pl.ds(place, length), pl.ds(number * hidden, hidden)],
                )
            )
    loads = [
        pltpu.make_async_copy(src, dst, r.load_sem.at[min(place, small + 1)])
        for place, (src, dst) in enumerate(pieces)
    ]
    for load in loads[:small]:
        load.start()

    down_loads = [
        pltpu.make_async_copy(
            r.down_hbm.at[:, columns], r.down.at[pl.ds(0, hidden), pl.ds(place, length)],
            r.load_sem.at[small + 2],
        )
        for columns, place, length in result_columns(c)
    ]

    barrier = pltpu.get_barrier_semaphore()
    for step in range(1, 2 * LINE):
        pl.semaphore_signal(
            barrier, inc=1, device_id=((e + step) % (2 * LINE), t), device_id_type=MESH
        )
    for other in (sibling, partner):
        pl.semaphore_signal(barrier, inc=1, device_id=other, device_id_type=MESH)

    for load in loads[:4]:
        load.wait()
    for load in loads[small:] + down_loads:
        load.start()
    widened = r.token[...].astype(jnp.float32)
    scale = lax.rsqrt(jnp.mean(widened * widened, axis=-1, keepdims=True) + EPS)
    r.own[...] = (widened * scale * r.gain[...]).astype(jnp.bfloat16)

    expert = lax.broadcasted_iota(jnp.int32, (2 * LINE, tokens), 0)
    named = jnp.zeros((2 * LINE, tokens), jnp.float32)
    for k in range(TOPK):
        named = named + jnp.where(expert == r.routing[k : k + 1], r.route_weight[k : k + 1], 0.0)
    r.shares[e] = named

    ahead = (
        lax.broadcasted_iota(jnp.int32, (tokens, tokens), 0)
        <= lax.broadcasted_iota(jnp.int32, (tokens, tokens), 1)
    ).astype(jnp.float32)
    slot = (lax.broadcasted_iota(jnp.int32, (SLOTS, tokens), 0) + 1).astype(jnp.float32)

    def ranked(block):
        routed = jnp.where(r.shares[block] > 0.0, 1.0, 0.0)
        r.ranks[block] = jnp.dot(routed, ahead, preferred_element_type=jnp.float32)

    def one_hot(block, expert):
        weight = r.shares[block, pl.ds(expert, 1), :]
        here = (r.ranks[block, pl.ds(expert, 1), :] == slot) & (weight > 0.0)
        return jnp.where(here, 1.0, 0.0), jnp.sum(jnp.where(here, weight, 0.0), axis=1, keepdims=True)

    def keep_weight(at, half, found):
        r.slot_weight[at, half * SLOTS : (half + 1) * SLOTS, :] = jnp.broadcast_to(found, (SLOTS, 128))

    def prepare(at):
        ranked(at * 2 + x)
        hot, found = one_hot(at * 2 + x, e)
        keep_weight(at, 0, found)
        r.hot[at, 0:SLOTS, :] = hot.astype(jnp.bfloat16)
        r.hot[at, SLOTS : 2 * SLOTS, :] = one_hot(at * 2 + x, z * 2 + 1 - x)[0].astype(jnp.bfloat16)

    def prepare_other(at):
        ranked(at * 2 + 1 - x)
        keep_weight(at, 1, one_hot(at * 2 + 1 - x, e)[1])

    for load in loads[4:small]:
        load.wait()
    pl.semaphore_wait(barrier, 2 * LINE + 1)

    parts = parts_of(lone, both)
    start_of_both = 2 * lone + c * both
    own_columns = (
        sections[0][0], aligned(start_of_both, both // 2), aligned(start_of_both + both // 2, both // 2)
    )

    def rows_of(half):
        return pl.ds(half * SLOTS, SLOTS)

    def own_along(up, part):
        start, length = parts[part]
        return copy(
            r.own.at[:, own_columns[part]], r.dense.at[z, :, pl.ds(start, length)],
            r.own_send.at[up], r.along_recv.at[z, part], (e + 4 * up - 2, t),
        )

    def onward(at, part):
        start, length = parts[part]
        view = r.dense.at[at, :, pl.ds(start, length)]
        to = (jnp.where(at < z, e + 2, e - 2), t)
        return copy(view, view, r.onward_send.at[at], r.along_recv.at[at, part], to)

    def across(at, part):
        start, length = parts[part]
        return copy(
            r.aside.at[at, :, pl.ds(start, length)],
            r.packed.at[at, rows_of(1), pl.ds(start, length)],
            r.across_send.at[at], r.across_recv.at[at, part], beside,
        )

    def to_partner(at, half):
        return copy(
            r.packed.at[at, rows_of(half), pl.ds(0, lone)],
            r.packed.at[at, rows_of(half), pl.ds(2 * held, lone)],
            r.partner_send.at[at], r.partner_recv.at[at, half], partner,
        )

    core_parts = [(start, held + start, length) for start, length in parts]
    core_parts.append((2 * held, 2 * held + lone, lone))

    def to_sibling(at, half, kind):
        start, landing, length = core_parts[kind]
        return copy(
            r.packed.at[at, rows_of(half), pl.ds(start, length)],
            r.packed.at[at, rows_of(half), pl.ds(landing, length)],
            r.core_send.at[at], r.core_recv.at[at], sibling,
        )

    def share_copy(step):
        to = (e + step) % (2 * LINE)
        return copy(r.shares.at[e], r.shares.at[e], r.share_send, r.share_recv.at[e], (to, t))

    def share_in(block):
        return copy(
            r.shares.at[block], r.shares.at[block], r.share_send, r.share_recv.at[block], beside
        )

    def own_along_start(part):
        @pl.when(z < LINE - 1)
        def _():
            own_along(1, part).start()

        @pl.when(z > 0)
        def _():
            own_along(0, part).start()

    def pack_aside(part):
        start, length = parts[part]
        found = jnp.dot(
            r.hot[z, SLOTS : 2 * SLOTS, :], r.own[:, own_columns[part]],
            preferred_element_type=jnp.float32,
        )
        r.aside[z, :, start : start + length] = found.astype(jnp.bfloat16)
        across(z, part).start()

    queries = r.query_hbm.shape[0]

    def halo_copy(which):
        src = (r.key, r.value)[which].at[pl.ds(queries - WINDOW_KEYS, WINDOW_KEYS)]
        to = ((e + 1) % (2 * LINE), t)
        return copy(src, r.halo.at[which], r.halo_send, r.halo_recv.at[which], to)

    @pl.when(e < 2 * LINE - 1)
    def _():
        halo_copy(0).start()
        halo_copy(1).start()

    @pl.when(e == 0)
    def _():
        r.halo[...] = jnp.zeros_like(r.halo)

    own_along_start(0)
    for step in range(1, 2 * LINE):
        share_copy(step).start()
    for part in range(1, len(parts)):
        own_along_start(part)
    prepare(z)
    for part in range(len(parts)):
        pack_aside(part)

    def down_copy(number):
        columns, place, length = result_columns(1 - c)[number]
        return copy(
            r.down_hbm.at[:, columns], r.down.at[pl.ds(hidden, hidden), pl.ds(place, length)],
            r.down_send, r.down_recv, sibling,
        )

    for number in range(3):
        down_copy(number).start()

    for columns, place, length in sections:
        found = jnp.dot(r.hot[z, 0:SLOTS, :], r.own[:, columns], preferred_element_type=jnp.float32)
        r.packed[z, 0:SLOTS, place : place + length] = found.astype(jnp.bfloat16)

    kv_heads = r.key_hbm.shape[1] // HEAD_SIZE
    group = r.query_hbm.shape[1] // HEAD_SIZE // kv_heads
    span = queries // 4
    here = lax.broadcasted_iota(jnp.int32, (WINDOW_KEYS, 2 * WINDOW_KEYS), 0)
    there = lax.broadcasted_iota(jnp.int32, (WINDOW_KEYS, 2 * WINDOW_KEYS), 1)

    def attend(number, kv):
        begin = number * WINDOW_KEYS
        permitted = (there > here) & (there <= here + WINDOW_KEYS)
        if number == 0:
            permitted = permitted & ((there >= WINDOW_KEYS) | (e > 0))
        lanes = slice(kv * HEAD_SIZE, (kv + 1) * HEAD_SIZE)
        if number == 0:
            keys = jnp.concatenate([r.halo[0][:, lanes], r.key[0:WINDOW_KEYS, lanes]], axis=0)
            values = jnp.concatenate([r.halo[1][:, lanes], r.value[0:WINDOW_KEYS, lanes]], axis=0)
        else:
            keys = r.key[begin - WINDOW_KEYS : begin + WINDOW_KEYS, lanes]
            values = r.value[begin - WINDOW_KEYS : begin + WINDOW_KEYS, lanes]
        for member in range(group):
            head = kv * group + member
            columns = slice(head * HEAD_SIZE, (head + 1) * HEAD_SIZE)
            scores = lax.dot_general(
                r.query[begin : begin + WINDOW_KEYS, columns],
                keys,
                (((1,), (1,)), ((), ())),
                preferred_element_type=jnp.float32,
            ) * HEAD_SIZE ** (-0.5)
            scores = jnp.where(permitted, scores, -jnp.inf)
            sink = r.sink[head]
            highest = jnp.maximum(jnp.max(scores, axis=-1, keepdims=True), sink)
            numerator = jnp.exp(scores - highest)
            denominator = jnp.sum(numerator, axis=-1, keepdims=True) + jnp.exp(sink - highest)
            weights = (numerator / denominator).astype(jnp.bfloat16)
            found = jnp.dot(weights, values, preferred_element_type=jnp.float32)
            r.attended[begin : begin + WINDOW_KEYS, columns] = found.astype(jnp.bfloat16)

    def halo_wait():
        @pl.when(e > 0)
        def _():
            halo_copy(0).wait_recv()
            halo_copy(1).wait_recv()

    def mixed_core(half):
        at = pl.multiple_of((half * 2 + 1 - c) * span, 16)
        return copy(
            r.mixed.at[pl.ds(at, span)], r.mixed_core.at[half],
            r.mixed_core_send, r.mixed_core_recv.at[half], sibling,
        )

    cut = span // MIXED_CUTS

    def mixed_pair(number):
        at = pl.multiple_of(((1 - y) * 2 + c) * span + number * cut, 16)
        return copy(
            r.mixed.at[pl.ds(at, cut)], r.mixed_pair.at[pl.ds(number * cut, cut)],
            r.mixed_pair_send, r.mixed_pair_recv.at[number], partner,
        )

    def mixed_rows(half):
        return pl.ds(pl.multiple_of((half * 2 + c) * span, 16), span)

    def mix():
        loads[small].wait()
        for place in range(0, width, quarter):
            columns = slice(place, place + quarter)
            r.mixed[:, columns] = jnp.dot(
                r.attended[...], r.project[:, columns], preferred_element_type=jnp.float32
            ).astype(jnp.bfloat16)
        for half in range(2):
            mixed_core(half).start()

    def mix_onward():
        for half in range(2):
            mixed_core(half).wait_recv()
            total = r.mixed[mixed_rows(half), :].astype(jnp.float32)
            r.mixed[mixed_rows(half), :] = (
                total + r.mixed_core[half].astype(jnp.float32)
            ).astype(jnp.bfloat16)

    def forward(k, part):
        onward(near[k], part).wait_recv()
        onward(near[k], part).start()

    def take_end(k, part):
        onward(near[k], part).wait_recv()

    def pack(k, part):
        at = near[k]
        start, length = parts[part]
        found = jnp.dot(
            r.hot[at], r.dense[at, :, start : start + length], preferred_element_type=jnp.float32
        ).astype(jnp.bfloat16)
        r.aside[at, :, start : start + length] = found[SLOTS : 2 * SLOTS]
        across(at, part).start()
        r.packed[at, 0:SLOTS, start : start + length] = found[0:SLOTS]
        if part == 0:
            to_partner(at, 0).start()
        to_sibling(at, 0, part).start()

    def take_across(k, part):
        at = near[k]
        across(at, part).wait_recv()
        if part == 0:
            to_partner(at, 1).start()
        to_sibling(at, 1, part).start()

    def take_partner(k, half):
        to_partner(near[k], half).wait_recv()
        to_sibling(near[k], half, len(parts)).start()

    def get_ready(k):
        share_in(near[k] * 2 + x).wait_recv()
        prepare(near[k])

    def get_other_ready(k):
        share_in(near[k] * 2 + 1 - x).wait_recv()
        prepare_other(near[k])

    def active_copy(at):
        return copy(
            r.active.at[at, :, pl.ds(0, hidden)], r.active.at[at, :, pl.ds(hidden, hidden)],
            r.active_send.at[at], r.active_recv.at[at], sibling,
        )

    def enter(k):
        at = near[k]
        rows = pl.ds(0, 2 * SLOTS) if k else pl.ds(0, SLOTS)
        arrived = r.packed.at[at, rows, pl.ds(0, held + lone)]
        copy(arrived, arrived, r.core_send.at[at], r.core_recv.at[at], sibling).wait_recv()
        pre = jnp.dot(r.packed[at], r.both_weights[...], preferred_element_type=jnp.float32)
        gate_cut = jnp.minimum(pre[:, 0:hidden], CLAMP)
        up_pre = pre[:, hidden : 2 * hidden]
        r.active[at, :, 0:hidden] = (
            (jnp.clip(up_pre, -CLAMP, CLAMP) + 1.0) * gate_cut * jax.nn.sigmoid(SLOPE * gate_cut)
        ).astype(jnp.bfloat16)
        active_copy(at).start()

    late = quarter - early
    chunks = chunks_of(quarter, early)

    def pair_copy(at, half):
        return copy(
            r.results.at[at, rows_of(half), pl.ds(carried, early)], r.pair.at[at, rows_of(half), :],
            r.pair_send.at[at], r.pair_recv.at[at, half], partner,
        )

    def side_copy(at, chunk):
        start, length = chunks[chunk]
        return copy(
            r.results.at[at, rows_of(1), pl.ds(start, length)], r.side.at[at, :, pl.ds(start, length)],
            r.side_send.at[at], r.side_recv.at[at, chunk], beside,
        )

    def leave(k):
        at = near[k]
        active_copy(at).wait_recv()

        def finish(start, length):
            found = jnp.dot(
                r.active[at], r.down[:, start : start + length], preferred_element_type=jnp.float32
            )
            r.results[at, :, start : start + length] = (found * r.slot_weight[at][:, 0:1]).astype(
                jnp.bfloat16
            )

        finish(carried, early)
        for chunk in range(2):
            finish(*chunks[chunk])
            if k:
                side_copy(at, chunk).start()
        finish(0, early)

    def send_pair(k, half):
        pair_copy(near[k], half).start()

    def send_side(k):
        side_copy(near[k], 0).start()
        side_copy(near[k], 1).start()

    def take_pair(k, half):
        at = near[k]
        pair_copy(at, half).wait_recv()
        rows = slice(half * SLOTS, (half + 1) * SLOTS)
        for chunk in range(2, len(chunks)):
            columns = slice(chunks[chunk][0], chunks[chunk][0] + chunks[chunk][1])
            total = r.results[at, rows, columns].astype(jnp.float32)
            r.results[at, rows, columns] = (
                total + r.pair[at, rows, columns].astype(jnp.float32)
            ).astype(jnp.bfloat16)
            if half:
                side_copy(at, chunk).start()

    def line_copy(way, at, chunk):
        start, length = chunks[chunk]
        to = (jnp.where(at > z, e + 2, e - 2), t)
        return copy(
            r.line_out.at[at, :, pl.ds(start, length)], r.line_in.at[way, at, :, pl.ds(start, length)],
            r.line_send.at[at], r.line_recv.at[way, at, chunk], to,
        )

    last = copy(r.line_out.at[z, :, pl.ds(quarter, late)], r.last, r.last_send, r.last_recv, partner)

    def line_step(k, chunk, middle):
        at = near[k]
        start, length = chunks[chunk]
        columns = slice(start, start + length)
        side_copy(at, chunk).wait_recv()
        both_sides = jnp.concatenate([r.results[at, 0:SLOTS, columns], r.side[at, :, columns]], axis=0)
        total = lax.dot_general(
            r.hot[at], both_sides, (((0,), (0,)), ((), ())), preferred_element_type=jnp.float32
        )
        if k:
            way = jnp.where(at > z, 0, 1)
            ways = (way,) if middle else ()
        elif middle:
            ways = (0, 1)
        else:
            ways = (jnp.where(z == 0, 1, 0),)
        for way in ways:
            line_copy(way, at, chunk).wait_recv()
            total = total + r.line_in[way, at, :, columns].astype(jnp.float32)
        if k or chunk == 0:
            r.line_out[at, :, columns] = total.astype(jnp.bfloat16)
            if k:
                line_copy(way, at, chunk).start()
            else:
                last.start()
        elif chunk == 1:
            r.final[...] = total
        else:
            r.out[:, columns] = total.astype(jnp.bfloat16)

    def wait_expert_weights():
        pltpu.make_async_copy(r.both_weights, r.both_weights, r.load_sem.at[small + 1]).wait()

    def wait_down_weights():
        arrived = r.down.at[pl.ds(0, hidden)]
        pltpu.make_async_copy(arrived, arrived, r.load_sem.at[small + 2]).wait()
        copy(arrived, arrived, r.down_send, r.down_recv, sibling).wait_recv()

    def send_mixed(number):
        mixed_pair(number).start()

    def finish_mixed():
        for number in range(MIXED_CUTS):
            mixed_pair(number).wait_recv()
        total = r.mixed[mixed_rows(y), :].astype(jnp.float32)
        r.mixer[...] = (total + r.mixed_pair[...].astype(jnp.float32)).astype(jnp.bfloat16)

    def at_places(which, *steps):
        @pl.when(which)
        def _():
            for step in steps:
                step[0](*step[1:])

    def sent(view, semaphore):
        copy(view, view, semaphore, semaphore, sibling).wait_send()

    def drain_dispatch():
        @pl.when(z < LINE - 1)
        def _():
            sent(r.dense.at[0], r.own_send.at[1])

        @pl.when(z > 0)
        def _():
            sent(r.dense.at[0], r.own_send.at[0])

        @pl.when(at_middle)
        def _():
            for k in range(1, LINE):
                sent(r.dense.at[near[k]], r.onward_send.at[near[k]])

        @pl.when(e < 2 * LINE - 1)
        def _():
            sent(r.halo, r.halo_send)

        sent(r.shares.at[pl.ds(0, 2 * LINE - 1)], r.share_send)
        sent(r.down.at[pl.ds(0, hidden)], r.down_send)
        sent(r.mixed_core, r.mixed_core_send)
        for k in range(LINE):
            at = near[k]
            sent(r.aside.at[at], r.across_send.at[at])
            rows = pl.ds(0, 2 * SLOTS) if k else pl.ds(0, SLOTS)
            sent(r.packed.at[at, rows, pl.ds(0, lone)], r.partner_send.at[at])
            sent(r.packed.at[at, rows, pl.ds(0, held + lone)], r.core_send.at[at])
            active_copy(at).wait_send()

    def drain_return():
        sent(r.mixed_pair, r.mixed_pair_send)
        for at in range(LINE):
            sent(r.pair.at[at], r.pair_send.at[at])
            sent(r.side.at[at], r.side_send.at[at])

    at_places(
        at_end,
        (take_across, 0, 0),
        (take_end, 1, 0),
    )
    get_ready(1)
    at_places(
        at_middle,
        (forward, 2, 0),
        (forward, 1, 0),
    )
    attend(1, 0)
    at_places(at_end, (take_end, 1, 1))
    pack(1, 0)
    halo_wait()
    attend(0, 1)
    at_places(
        at_end,
        (take_across, 0, 2),
        (pack, 1, 1),
    )
    attend(1, 1)
    at_places(at_end, (take_partner, 0, 1))
    at_places(at_middle, (take_across, 0, 0))
    get_other_ready(0)
    attend(0, 0)
    at_places(at_end, (take_across, 1, 0))
    at_places(at_middle, (forward, 1, 1))
    get_ready(2)
    mix()
    at_places(at_end, (take_end, 2, 0))
    at_places(at_middle, (pack, 1, 1))
    pack(2, 0)
    at_places(
        at_middle,
        (take_across, 0, 2),
        (forward, 2, 1),
    )
    get_other_ready(1)
    at_places(at_end, (take_across, 0, 1))
    at_places(at_middle, (forward, 3, 0))
    get_ready(3)
    at_places(
        at_end,
        (take_partner, 1, 0),
        (take_end, 2, 1),
    )
    at_places(
        at_middle,
        (pack, 2, 1),
        (pack, 3, 0),
        (take_across, 0, 1),
        (forward, 2, 2),
    )
    mix_onward()
    at_places(
        at_end,
        (take_end, 1, 2),
        (send_mixed, 1),
        (pack, 1, 2),
    )
    at_places(
        at_middle,
        (forward, 3, 1),
        (take_across, 1, 1),
        (take_across, 1, 0),
        (pack, 2, 2),
        (take_partner, 0, 1),
        (take_across, 2, 0),
        (forward, 3, 2),
        (take_partner, 3, 0),
    )
    get_other_ready(2)
    at_places(at_middle, (take_across, 3, 0))
    get_other_ready(3)
    at_places(
        at_end,
        (take_end, 3, 0),
        (pack, 3, 0),
    )
    at_places(
        at_middle,
        (take_across, 2, 1),
        (take_partner, 1, 1),
        (forward, 1, 2),
        (send_mixed, 0),
        (pack, 3, 1),
    )
    wait_expert_weights()
    enter(0)
    at_places(
        at_end,
        (pack, 2, 1),
        (take_across, 2, 0),
        (take_across, 1, 1),
        (take_partner, 1, 1),
    )
    at_places(
        at_middle,
        (pack, 1, 2),
        (take_partner, 2, 0),
        (take_partner, 1, 0),
        (take_partner, 2, 1),
    )
    wait_down_weights()
    leave(0)
    at_places(
        at_middle,
        (take_across, 3, 1),
        (send_pair, 0, 1),
        (take_partner, 3, 1),
        (take_across, 2, 2),
        (pack, 3, 2),
        (send_side, 0),
        (send_pair, 0, 0),
    )
    take_across(1, 2)
    at_places(
        at_end,
        (take_end, 3, 1),
        (take_across, 3, 0),
        (send_mixed, 0),
        (pack, 3, 1),
        (take_partner, 3, 0),
        (take_end, 3, 2),
        (pack, 3, 2),
    )
    enter(1)
    at_places(at_end, (send_pair, 0, 0))
    at_places(at_middle, (take_across, 3, 2))
    leave(1)
    at_places(
        at_end,
        (take_across, 3, 1),
        (take_end, 2, 2),
    )
    send_pair(1, 1)
    at_places(
        at_end,
        (pack, 2, 2),
        (take_partner, 3, 1),
        (take_partner, 2, 1),
        (take_across, 3, 2),
    )
    enter(3)
    at_places(
        at_end,
        (take_partner, 2, 0),
        (take_across, 2, 1),
        (line_step, 1, 0, False),
    )
    at_places(at_middle, (send_pair, 1, 0))
    leave(3)
    at_places(
        at_end,
        (line_step, 1, 1, False),
        (send_pair, 3, 1),
    )
    at_places(at_middle, (take_pair, 0, 0))
    send_pair(3, 0)
    at_places(at_end, (take_across, 2, 2))
    enter(2)
    at_places(at_end, (line_step, 3, 0, False))
    leave(2)
    at_places(
        at_middle,
        (send_pair, 3, 1),
        (line_step, 3, 0, True),
        (take_pair, 3, 0),
        (send_pair, 2, 1),
        (line_step, 3, 1, True),
        (take_pair, 3, 1),
        (send_mixed, 2),
        (take_pair, 1, 0),
        (take_pair, 1, 1),
        (line_step, 2, 0, True),
        (line_step, 1, 0, True),
    )
    send_pair(2, 0)
    at_places(
        at_end,
        (line_step, 3, 1, False),
        (send_pair, 2, 1),
        (send_pair, 1, 0),
        (take_pair, 3, 1),
        (line_step, 2, 0, False),
        (take_pair, 3, 0),
        (take_pair, 0, 0),
        (line_step, 2, 1, False),
    )
    at_places(at_middle, (line_step, 1, 1, True))
    send_mixed(3)
    at_places(
        at_end,
        (send_pair, 0, 1),
        (send_mixed, 2),
        (line_step, 3, 2, False),
    )
    at_places(at_middle, (send_mixed, 1))
    take_pair(2, 1)
    at_places(
        at_end,
        (take_pair, 1, 1),
        (line_step, 3, 3, False),
    )
    at_places(
        at_middle,
        (line_step, 3, 2, True),
        (line_step, 2, 1, True),
        (take_pair, 0, 1),
        (line_step, 0, 0, True),
    )
    take_pair(2, 0)
    at_places(
        at_end,
        (take_pair, 1, 0),
        (line_step, 2, 2, False),
        (line_step, 2, 3, False),
        (send_side, 0),
        (line_step, 1, 2, False),
        (line_step, 1, 3, False),
        (take_pair, 0, 1),
        (line_step, 0, 0, False),
        (line_step, 0, 2, False),
    )
    at_places(
        at_middle,
        (line_step, 3, 3, True),
        (line_step, 0, 1, True),
        (line_step, 1, 2, True),
        (line_step, 2, 2, True),
    )
    drain_dispatch()
    at_places(at_end, (line_step, 0, 1, False))
    at_places(
        at_middle,
        (line_step, 1, 3, True),
        (line_step, 2, 3, True),
    )
    finish_mixed()
    at_places(at_end, (line_step, 0, 3, False))
    at_places(
        at_middle,
        (line_step, 0, 2, True),
        (line_step, 0, 3, True),
    )
    drain_return()

    last.wait_recv()
    r.out[:, early:quarter] = (r.final[...] + r.last[...].astype(jnp.float32)).astype(
        jnp.bfloat16
    )
    last.wait_send()
    for k in range(1, LINE):
        sent(r.line_out.at[near[k]], r.line_send.at[near[k]])


def layer_call(
    rows, gain, routing, route_weight, queries, keys, values, sinks, project, gate_one, up_one, down_one
):
    tokens, width = rows.shape
    quarter, lone, both, early, carried = sizes_of(width)
    parts, chunks = len(parts_of(lone, both)), len(chunks_of(quarter, early))
    blocks = 2 * LINE
    hidden = gate_one.shape[1]
    kept = jnp.bfloat16
    dma = pltpu.SemaphoreType.DMA
    span = queries.shape[0] // 4
    stays = pl.BlockSpec(memory_space=pl.ANY)
    in_vmem = pl.BlockSpec(memory_space=pltpu.VMEM)
    scratch = dict(
        token=pltpu.VMEM(rows.shape, kept),
        gain=pltpu.VMEM(gain.shape, jnp.float32),
        routing=pltpu.VMEM(routing.shape, jnp.int32),
        route_weight=pltpu.VMEM(route_weight.shape, jnp.float32),
        query=pltpu.VMEM(queries.shape, kept),
        key=pltpu.VMEM(keys.shape, kept),
        value=pltpu.VMEM(values.shape, kept),
        sink=pltpu.SMEM(sinks.shape, jnp.float32),
        own=pltpu.VMEM((tokens, width), kept),
        dense=pltpu.VMEM((LINE, tokens, lone + both), kept),
        packed=pltpu.VMEM((LINE, 2 * SLOTS, width), kept),
        aside=pltpu.VMEM((LINE, SLOTS, lone + both), kept),
        both_weights=pltpu.VMEM((width, 2 * hidden), kept),
        down=pltpu.VMEM((2 * hidden, 2 * quarter), kept),
        project=pltpu.VMEM(project.shape, kept),
        halo=pltpu.VMEM((2, WINDOW_KEYS, keys.shape[1]), kept),
        attended=pltpu.VMEM(queries.shape, kept),
        mixed=pltpu.VMEM((queries.shape[0], width), kept),
        mixed_core=pltpu.VMEM((2, span, width), kept),
        mixed_pair=pltpu.VMEM((span, width), kept),
        shares=pltpu.VMEM((blocks, 8, tokens), jnp.float32),
        ranks=pltpu.VMEM((blocks, 8, tokens), jnp.float32),
        hot=pltpu.VMEM((LINE, 2 * SLOTS, tokens), kept),
        slot_weight=pltpu.VMEM((LINE, 2 * SLOTS, 128), jnp.float32),
        active=pltpu.VMEM((LINE, 2 * SLOTS, 2 * hidden), kept),
        results=pltpu.VMEM((LINE, 2 * SLOTS, 2 * quarter), kept),
        pair=pltpu.VMEM((LINE, 2 * SLOTS, early), kept),
        side=pltpu.VMEM((LINE, SLOTS, carried), kept),
        line_out=pltpu.VMEM((LINE, tokens, carried), kept),
        line_in=pltpu.VMEM((2, LINE, tokens, carried), kept),
        last=pltpu.VMEM((tokens, quarter - early), kept),
        final=pltpu.VMEM((tokens, quarter - early), jnp.float32),
        load_sem=dma((11,)),
        halo_send=dma,
        halo_recv=dma((2,)),
        mixed_core_send=dma,
        mixed_core_recv=dma((2,)),
        mixed_pair_send=dma,
        mixed_pair_recv=dma((MIXED_CUTS,)),
        share_send=dma,
        share_recv=dma((blocks,)),
        own_send=dma((2,)),
        onward_send=dma((LINE,)),
        along_recv=dma((LINE, parts)),
        across_send=dma((LINE,)),
        across_recv=dma((LINE, parts)),
        partner_send=dma((LINE,)),
        partner_recv=dma((LINE, 2)),
        core_send=dma((LINE,)),
        core_recv=dma((LINE,)),
        down_send=dma,
        down_recv=dma,
        active_send=dma((LINE,)),
        active_recv=dma((LINE,)),
        pair_send=dma((LINE,)),
        pair_recv=dma((LINE, 2)),
        side_send=dma((LINE,)),
        side_recv=dma((LINE, chunks)),
        line_send=dma((LINE,)),
        line_recv=dma((2, LINE, chunks)),
        last_send=dma,
        last_recv=dma,
    )
    return pl.pallas_call(
        layer_kernel,
        out_shape=(
            pltpu.VMEM((span, width), kept),
            pltpu.VMEM((tokens, quarter), kept),
        ),
        in_specs=[stays] * 12,
        out_specs=(in_vmem, in_vmem),
        scratch_shapes=[scratch[name] for name in NAMES[14:]],
        compiler_params=pltpu.CompilerParams(
            collective_id=0, has_side_effects=True, vmem_limit_bytes=60 * 1024 * 1024
        ),
        cost_estimate=pl.CostEstimate(
            flops=8 * blocks * tokens * width * hidden,
            bytes_accessed=8 * width * hidden,
            transcendentals=0,
        ),
    )(rows, gain, routing, route_weight, queries, keys, values, sinks, project, gate_one, up_one, down_one)


def shards(
    projected_queries,
    key_proj,
    projected_values,
    head_sink_logits,
    out_weight,
    expert_input,
    norm_gain,
    routing,
    route_weight,
    gate_weight,
    up_weight,
    down_weight,
):
    token_rows = expert_input.shape[0]
    experts = lax.axis_size("ep")
    capacity = max(3 * token_rows * TOPK // (2 * experts), 2)
    col_share = D // lax.axis_size("tp")
    if (experts, lax.axis_size("tp")) == (2 * LINE, 4) and token_rows == 128:
        return layer_call(
            expert_input,
            norm_gain[None, :],
            routing.T,
            route_weight.T,
            projected_queries,
            key_proj,
            projected_values,
            head_sink_logits,
            out_weight,
            gate_weight[0],
            up_weight[0],
            down_weight[0],
        )
    widened = expert_input.astype(jnp.float32)
    normed = (
        widened
        * lax.rsqrt(jnp.mean(widened * widened, axis=-1, keepdims=True) + EPS)
        * norm_gain[None, :]
    ).astype(jnp.bfloat16)
    query_rows = projected_queries.shape[0]
    kv_heads = key_proj.shape[1] // HEAD_SIZE
    heads_per_group = projected_queries.shape[1] // HEAD_SIZE // kv_heads
    count_of_blocks = query_rows // WINDOW_KEYS
    prior_key, prior_value = passed_along(
        (key_proj[query_rows - WINDOW_KEYS :], projected_values[query_rows - WINDOW_KEYS :]),
        "ep",
        1,
    )
    key_all = jnp.concatenate([prior_key, key_proj], axis=0)
    value_all = jnp.concatenate([prior_value, projected_values], axis=0)
    window_keys = jnp.concatenate(
        [
            key_all[:-WINDOW_KEYS].reshape(count_of_blocks, WINDOW_KEYS, kv_heads, HEAD_SIZE),
            key_all[WINDOW_KEYS:].reshape(count_of_blocks, WINDOW_KEYS, kv_heads, HEAD_SIZE),
        ],
        axis=1,
    )
    window_values = jnp.concatenate(
        [
            value_all[:-WINDOW_KEYS].reshape(count_of_blocks, WINDOW_KEYS, kv_heads, HEAD_SIZE),
            value_all[WINDOW_KEYS:].reshape(count_of_blocks, WINDOW_KEYS, kv_heads, HEAD_SIZE),
        ],
        axis=1,
    )
    query_blocks = projected_queries.reshape(
        count_of_blocks, WINDOW_KEYS, kv_heads, heads_per_group, HEAD_SIZE
    )
    scores = jnp.einsum(
        "nqhgd,nshd->nhgqs", query_blocks, window_keys, preferred_element_type=jnp.float32
    ) * HEAD_SIZE ** (-0.5)
    offset = lax.axis_index("ep") * query_rows
    block_ids = jnp.arange(count_of_blocks)[:, None, None] * WINDOW_KEYS + offset
    query_pos = block_ids + jnp.arange(WINDOW_KEYS)[None, :, None]
    key_pos = block_ids - WINDOW_KEYS + jnp.arange(2 * WINDOW_KEYS)[None, None, :]
    permitted_mask = (key_pos <= query_pos) & (query_pos - key_pos < WINDOW_KEYS) & (key_pos >= 0)
    scores = jnp.where(permitted_mask[:, None, None, :, :], scores, -jnp.inf)
    sink_col = head_sink_logits.reshape(kv_heads, heads_per_group)[None, :, :, None, None]
    highest = jnp.maximum(jnp.max(scores, axis=-1, keepdims=True), sink_col)
    numerator = jnp.exp(scores - highest)
    denominator = jnp.sum(numerator, axis=-1, keepdims=True) + jnp.exp(sink_col - highest)
    weights = (numerator / denominator).astype(jnp.bfloat16)
    attended = jnp.einsum(
        "nhgqs,nshd->nqhgd", weights, window_values, preferred_element_type=jnp.float32
    )
    attended = attended.astype(jnp.bfloat16).reshape(
        query_rows, kv_heads * heads_per_group * HEAD_SIZE
    )
    mixer_output = lax.psum_scatter(
        jnp.dot(attended, out_weight, preferred_element_type=jnp.float32).astype(jnp.bfloat16),
        "tp",
        scatter_dimension=0,
        tiled=True,
    )
    flat_ids = routing.reshape(-1)
    onehot = (flat_ids[:, None] == jnp.arange(experts, dtype=jnp.int32)[None, :]).astype(jnp.int32)
    rank_in = jnp.cumsum(onehot, axis=0) - 1
    target = flat_ids * capacity + jnp.sum(rank_in * onehot, axis=1)
    tok_ids = jnp.arange(token_rows * TOPK) // TOPK
    slot_tok = jnp.full((experts * capacity,), token_rows, jnp.int32).at[target].set(tok_ids)
    gate_one = gate_weight[0]
    up_one = up_weight[0]
    own_cols = lax.dynamic_slice_in_dim(normed, lax.axis_index("tp") * col_share, col_share, 1)
    extended = jnp.concatenate([own_cols, jnp.zeros((1, col_share), jnp.bfloat16)], axis=0)
    outgoing = jnp.take(extended, slot_tok, axis=0).reshape(experts, capacity, col_share)
    arrived = lax.all_to_all(outgoing, "ep", split_axis=0, concat_axis=0, tiled=True).reshape(
        experts * capacity, col_share
    )
    portion = lax.all_gather(arrived, "tp", axis=1, tiled=True)
    gate_pre = jnp.dot(portion, gate_one, preferred_element_type=jnp.float32)
    up_pre = jnp.dot(portion, up_one, preferred_element_type=jnp.float32)
    gate_cut = jnp.minimum(gate_pre, CLAMP)
    activated = (
        (jnp.clip(up_pre, -CLAMP, CLAMP) + 1.0) * gate_cut * jax.nn.sigmoid(SLOPE * gate_cut)
    ).astype(jnp.bfloat16)
    partial_value = jnp.dot(activated, down_weight[0], preferred_element_type=jnp.float32)
    expert_result = lax.psum_scatter(
        partial_value.astype(jnp.bfloat16), "tp", scatter_dimension=1, tiled=True
    )
    returned = lax.all_to_all(
        expert_result.reshape(experts, capacity, col_share),
        "ep",
        split_axis=0,
        concat_axis=0,
        tiled=True,
    )
    picked = jnp.take(returned.reshape(experts * capacity, col_share), target, axis=0)
    picked = picked.astype(jnp.float32).reshape(token_rows, TOPK, col_share)
    expert_output = jnp.sum(picked * route_weight[:, :, None], axis=1).astype(jnp.bfloat16)
    return (mixer_output, expert_output)


def solution(mesh):
    placed = (
        P("ep", "tp"),
        P("ep", "tp"),
        P("ep", "tp"),
        P("tp"),
        P("tp", None),
        P("ep", None),
        P(),
        P("ep", None),
        P("ep", None),
        P("ep", None, "tp"),
        P("ep", None, "tp"),
        P("ep", "tp", None),
    )
    return jax.shard_map(
        shards,
        mesh=mesh,
        in_specs=placed,
        out_specs=(P(("ep", "tp"), None), P("ep", "tp")),
        check_vma=False,
    )
```

```python
import types

import jax
import jax.numpy as jnp
from jax import lax
from jax.experimental import pallas as pl
from jax.experimental.pallas import tpu as pltpu
from jax.sharding import PartitionSpec as P

D = 4096
HEAD_SIZE = 64
WINDOW_KEYS = 128
TOPK = 4


EPS = 1e-06
CLAMP = 7.0
SLOPE = 1.702


def passed_along(block, axis, distance):
    devices = range(lax.axis_size(axis))
    route = [(i - distance, i) for i in devices if i - distance in devices]
    return lax.ppermute(block, axis, route)


LINE = 4
SLOTS = 96
LONE = 4
EARLY = 5
MIXED_CUTS = 4
MESH = pl.DeviceIdType.MESH

NAMES = (
    "token_hbm", "gain_hbm", "routing_hbm", "route_weight_hbm", "query_hbm", "key_hbm",
    "value_hbm", "sink_hbm", "project_hbm", "gate_hbm", "up_hbm", "down_hbm", "mixer", "out",
    "token", "gain", "routing", "route_weight", "query", "key", "value", "sink", "own", "dense",
    "packed", "aside", "both_weights", "down", "project", "halo", "attended", "mixed",
    "mixed_core", "mixed_pair", "shares", "ranks", "hot", "slot_weight", "active", "results",
    "pair", "side", "line_out", "line_in", "last", "final", "load_sem", "halo_send", "halo_recv",
    "mixed_core_send", "mixed_core_recv", "mixed_pair_send", "mixed_pair_recv", "share_send",
    "share_recv", "own_send", "onward_send", "along_recv", "across_send", "across_recv",
    "partner_send", "partner_recv", "core_send", "core_recv", "down_send", "down_recv",
    "active_send", "active_recv", "pair_send", "pair_recv", "side_send", "side_recv", "line_send",
    "line_recv", "last_send", "last_recv",
)


def chosen(z, values):
    result = jnp.int32(values[0])
    for place in range(1, LINE):
        result = jnp.where(z == place, jnp.int32(values[place]), result)
    return result


def nearest_first(place):
    return sorted(range(LINE), key=lambda other: (abs(other - place), abs(2 * other - LINE + 1)))


def sizes_of(width):
    quarter = width // 4
    lone = width * LONE // 32
    both = (width - 4 * lone) // 2
    early = width * EARLY // 32
    return quarter, lone, both, early, 2 * quarter - early


def parts_of(lone, both):
    return (0, lone), (lone, both // 2), (lone + both // 2, both // 2)


def chunks_of(quarter, early):
    late = quarter - early
    cut = (early + 128) // 256 * 128
    return (quarter, late), (early, late), (0, cut), (cut, early - cut)


def layer_kernel(*refs):
    r = types.SimpleNamespace(**dict(zip(NAMES, refs)))
    e, t = lax.axis_index("ep"), lax.axis_index("tp")
    z, x, y, c = e // 2, e % 2, t // 2, t % 2
    tokens, width = r.token_hbm.shape
    quarter, lone, both, early, carried = sizes_of(width)
    held = lone + both
    hidden = r.gate_hbm.shape[1]
    sibling, partner, beside = (e, y * 2 + 1 - c), (e, (1 - y) * 2 + c), (z * 2 + 1 - x, t)
    at_end = (z == 0) | (z == LINE - 1)
    at_middle = (z > 0) & (z < LINE - 1)
    near = [chosen(z, [nearest_first(place)[j] for place in range(LINE)]) for j in range(LINE)]

    def copy(src, dst, send, recv, to):
        return pltpu.make_async_remote_copy(
            src_ref=src, dst_ref=dst, send_sem=send, recv_sem=recv, device_id=to, device_id_type=MESH
        )

    def aligned(start, length):
        return pl.ds(pl.multiple_of(start, 128), length)

    def lone_of(row, core):
        return aligned(row * (width - 2 * lone) + core * lone, lone)

    def both_of(core):
        return aligned(2 * lone + core * both, both)

    sections = [
        (lone_of(y, c), 0, lone),
        (both_of(c), lone, both),
        (lone_of(y, 1 - c), held, lone),
        (both_of(1 - c), held + lone, both),
        (lone_of(1 - y, c), 2 * held, lone),
        (lone_of(1 - y, 1 - c), 2 * held + lone, lone),
    ]
    mine, theirs = (y * 2 + c) * quarter, ((1 - y) * 2 + c) * quarter

    def result_columns(core):
        own, other = (y * 2 + core) * quarter, ((1 - y) * 2 + core) * quarter
        return [
            (aligned(own, quarter), 0, quarter),
            (aligned(other + early, quarter - early), quarter, quarter - early),
            (aligned(other, early), carried, early),
        ]

    pieces = [
        (r.token_hbm, r.token), (r.gain_hbm, r.gain), (r.routing_hbm, r.routing),
        (r.route_weight_hbm, r.route_weight), (r.sink_hbm, r.sink), (r.query_hbm, r.query), (r.key_hbm, r.key),
        (r.value_hbm, r.value), (r.project_hbm, r.project),
    ]
    small = len(pieces) - 1
    for columns, place, length in sections:
        for number, weights in enumerate((r.gate_hbm, r.up_hbm)):
            pieces.append(
                (
                    weights.at[columns, :],
                    r.both_weights.at[pl.ds(place, length), pl.ds(number * hidden, hidden)],
                )
            )
    loads = [
        pltpu.make_async_copy(src, dst, r.load_sem.at[min(place, small + 1)])
        for place, (src, dst) in enumerate(pieces)
    ]
    for load in loads[:small]:
        load.start()

    down_loads = [
        pltpu.make_async_copy(
            r.down_hbm.at[:, columns], r.down.at[pl.ds(0, hidden), pl.ds(place, length)],
            r.load_sem.at[small + 2],
        )
        for columns, place, length in result_columns(c)
    ]

    barrier = pltpu.get_barrier_semaphore()
    for step in range(1, 2 * LINE):
        pl.semaphore_signal(
            barrier, inc=1, device_id=((e + step) % (2 * LINE), t), device_id_type=MESH
        )
    for other in (sibling, partner):
        pl.semaphore_signal(barrier, inc=1, device_id=other, device_id_type=MESH)

    for load in loads[:2]:
        load.wait()
    for load in loads[small:] + down_loads:
        load.start()
    widened = r.token[...].astype(jnp.float32)
    scale = lax.rsqrt(jnp.mean(widened * widened, axis=-1, keepdims=True) + EPS)
    r.own[...] = (widened * scale * r.gain[...]).astype(jnp.bfloat16)

    for load in loads[2:4]:
        load.wait()
    expert = lax.broadcasted_iota(jnp.int32, (2 * LINE, tokens), 0)
    named = jnp.zeros((2 * LINE, tokens), jnp.float32)
    for k in range(TOPK):
        named = named + jnp.where(expert == r.routing[k : k + 1], r.route_weight[k : k + 1], 0.0)
    r.shares[e] = named

    ahead = (
        lax.broadcasted_iota(jnp.int32, (tokens, tokens), 0)
        <= lax.broadcasted_iota(jnp.int32, (tokens, tokens), 1)
    ).astype(jnp.float32)
    slot = (lax.broadcasted_iota(jnp.int32, (SLOTS, tokens), 0) + 1).astype(jnp.float32)

    def ranked(block):
        routed = jnp.where(r.shares[block] > 0.0, 1.0, 0.0)
        r.ranks[block] = jnp.dot(routed, ahead, preferred_element_type=jnp.float32)

    def one_hot(block, expert):
        weight = r.shares[block, pl.ds(expert, 1), :]
        here = (r.ranks[block, pl.ds(expert, 1), :] == slot) & (weight > 0.0)
        return jnp.where(here, 1.0, 0.0), jnp.sum(jnp.where(here, weight, 0.0), axis=1, keepdims=True)

    def keep_weight(at, half, found):
        r.slot_weight[at, half * SLOTS : (half + 1) * SLOTS, :] = jnp.broadcast_to(found, (SLOTS, 128))

    def prepare(at):
        ranked(at * 2 + x)
        hot, found = one_hot(at * 2 + x, e)
        keep_weight(at, 0, found)
        r.hot[at, 0:SLOTS, :] = hot.astype(jnp.bfloat16)
        r.hot[at, SLOTS : 2 * SLOTS, :] = one_hot(at * 2 + x, z * 2 + 1 - x)[0].astype(jnp.bfloat16)

    def prepare_other(at):
        ranked(at * 2 + 1 - x)
        keep_weight(at, 1, one_hot(at * 2 + 1 - x, e)[1])

    for load in loads[4:small]:
        load.wait()
    pl.semaphore_wait(barrier, 2 * LINE + 1)

    parts = parts_of(lone, both)
    start_of_both = 2 * lone + c * both
    own_columns = (
        sections[0][0], aligned(start_of_both, both // 2), aligned(start_of_both + both // 2, both // 2)
    )

    def rows_of(half):
        return pl.ds(half * SLOTS, SLOTS)

    def own_along(up, part):
        start, length = parts[part]
        return copy(
            r.own.at[:, own_columns[part]], r.dense.at[z, :, pl.ds(start, length)],
            r.own_send.at[up], r.along_recv.at[z, part], (e + 4 * up - 2, t),
        )

    def onward(at, part):
        start, length = parts[part]
        view = r.dense.at[at, :, pl.ds(start, length)]
        to = (jnp.where(at < z, e + 2, e - 2), t)
        return copy(view, view, r.onward_send, r.along_recv.at[at, part], to)

    def across(at, part):
        start, length = parts[part]
        return copy(
            r.aside.at[at, :, pl.ds(start, length)],
            r.packed.at[at, rows_of(1), pl.ds(start, length)],
            r.across_send, r.across_recv.at[at, part], beside,
        )

    def to_partner(at, half):
        return copy(
            r.packed.at[at, rows_of(half), pl.ds(0, lone)],
            r.packed.at[at, rows_of(half), pl.ds(2 * held, lone)],
            r.partner_send.at[at], r.partner_recv.at[at, half], partner,
        )

    core_parts = [(start, held + start, length) for start, length in parts]
    core_parts.append((2 * held, 2 * held + lone, lone))

    def to_sibling(at, half, kind):
        start, landing, length = core_parts[kind]
        return copy(
            r.packed.at[at, rows_of(half), pl.ds(start, length)],
            r.packed.at[at, rows_of(half), pl.ds(landing, length)],
            r.core_send.at[at], r.core_recv.at[at], sibling,
        )

    def share_copy(step):
        to = (e + step) % (2 * LINE)
        return copy(r.shares.at[e], r.shares.at[e], r.share_send, r.share_recv.at[e], (to, t))

    def share_in(block):
        return copy(
            r.shares.at[block], r.shares.at[block], r.share_send, r.share_recv.at[block], beside
        )

    def own_along_start(part):
        @pl.when(z < LINE - 1)
        def _():
            own_along(1, part).start()

        @pl.when(z > 0)
        def _():
            own_along(0, part).start()

    def pack_aside(part):
        start, length = parts[part]
        found = jnp.dot(
            r.hot[z, SLOTS : 2 * SLOTS, :], r.own[:, own_columns[part]],
            preferred_element_type=jnp.float32,
        )
        r.aside[z, :, start : start + length] = found.astype(jnp.bfloat16)
        across(z, part).start()

    queries = r.query_hbm.shape[0]

    def halo_copy(which):
        src = (r.key, r.value)[which].at[pl.ds(queries - WINDOW_KEYS, WINDOW_KEYS)]
        to = ((e + 1) % (2 * LINE), t)
        return copy(src, r.halo.at[which], r.halo_send, r.halo_recv.at[which], to)

    @pl.when(e < 2 * LINE - 1)
    def _():
        halo_copy(0).start()
        halo_copy(1).start()

    @pl.when(e == 0)
    def _():
        r.halo[...] = jnp.zeros_like(r.halo)

    own_along_start(0)
    for step in range(1, 2 * LINE):
        share_copy(step).start()
    for part in range(1, len(parts)):
        own_along_start(part)
    prepare(z)
    for part in range(len(parts)):
        pack_aside(part)

    def down_copy(number):
        columns, place, length = result_columns(1 - c)[number]
        return copy(
            r.down_hbm.at[:, columns], r.down.at[pl.ds(hidden, hidden), pl.ds(place, length)],
            r.down_send, r.down_recv, sibling,
        )

    for number in range(3):
        down_copy(number).start()

    for columns, place, length in sections:
        found = jnp.dot(r.hot[z, 0:SLOTS, :], r.own[:, columns], preferred_element_type=jnp.float32)
        r.packed[z, 0:SLOTS, place : place + length] = found.astype(jnp.bfloat16)

    kv_heads = r.key_hbm.shape[1] // HEAD_SIZE
    group = r.query_hbm.shape[1] // HEAD_SIZE // kv_heads
    span = queries // 4
    here = lax.broadcasted_iota(jnp.int32, (WINDOW_KEYS, 2 * WINDOW_KEYS), 0)
    there = lax.broadcasted_iota(jnp.int32, (WINDOW_KEYS, 2 * WINDOW_KEYS), 1)

    def attend(number, kv):
        begin = number * WINDOW_KEYS
        permitted = (there > here) & (there <= here + WINDOW_KEYS)
        if number == 0:
            permitted = permitted & ((there >= WINDOW_KEYS) | (e > 0))
        lanes = slice(kv * HEAD_SIZE, (kv + 1) * HEAD_SIZE)
        if number == 0:
            keys = jnp.concatenate([r.halo[0][:, lanes], r.key[0:WINDOW_KEYS, lanes]], axis=0)
            values = jnp.concatenate([r.halo[1][:, lanes], r.value[0:WINDOW_KEYS, lanes]], axis=0)
        else:
            keys = r.key[begin - WINDOW_KEYS : begin + WINDOW_KEYS, lanes]
            values = r.value[begin - WINDOW_KEYS : begin + WINDOW_KEYS, lanes]
        for member in range(group):
            head = kv * group + member
            columns = slice(head * HEAD_SIZE, (head + 1) * HEAD_SIZE)
            scores = lax.dot_general(
                r.query[begin : begin + WINDOW_KEYS, columns],
                keys,
                (((1,), (1,)), ((), ())),
                preferred_element_type=jnp.float32,
            ) * HEAD_SIZE ** (-0.5)
            scores = jnp.where(permitted, scores, -jnp.inf)
            sink = r.sink[head]
            highest = jnp.maximum(jnp.max(scores, axis=-1, keepdims=True), sink)
            numerator = jnp.exp(scores - highest)
            denominator = jnp.sum(numerator, axis=-1, keepdims=True) + jnp.exp(sink - highest)
            weights = (numerator / denominator).astype(jnp.bfloat16)
            found = jnp.dot(weights, values, preferred_element_type=jnp.float32)
            r.attended[begin : begin + WINDOW_KEYS, columns] = found.astype(jnp.bfloat16)

    def halo_wait():
        @pl.when(e > 0)
        def _():
            halo_copy(0).wait_recv()
            halo_copy(1).wait_recv()

    def mixed_core(half):
        at = pl.multiple_of((half * 2 + 1 - c) * span, 16)
        return copy(
            r.mixed.at[pl.ds(at, span)], r.mixed_core.at[half],
            r.mixed_core_send, r.mixed_core_recv.at[half], sibling,
        )

    cut = span // MIXED_CUTS

    def mixed_pair(number):
        at = pl.multiple_of(((1 - y) * 2 + c) * span + number * cut, 16)
        return copy(
            r.mixed.at[pl.ds(at, cut)], r.mixed_pair.at[pl.ds(number * cut, cut)],
            r.mixed_pair_send, r.mixed_pair_recv, partner,
        )

    def mixed_rows(half):
        return pl.ds(pl.multiple_of((half * 2 + c) * span, 16), span)

    def mix():
        loads[small].wait()
        for place in range(0, width, quarter):
            columns = slice(place, place + quarter)
            r.mixed[:, columns] = jnp.dot(
                r.attended[...], r.project[:, columns], preferred_element_type=jnp.float32
            ).astype(jnp.bfloat16)
        for half in range(2):
            mixed_core(half).start()

    def mix_onward():
        for half in range(2):
            mixed_core(half).wait_recv()
            total = r.mixed[mixed_rows(half), :].astype(jnp.float32)
            r.mixed[mixed_rows(half), :] = (
                total + r.mixed_core[half].astype(jnp.float32)
            ).astype(jnp.bfloat16)

    def forward(k, part):
        onward(near[k], part).wait_recv()
        onward(near[k], part).start()

    def take_end(k, part):
        onward(near[k], part).wait_recv()

    def pack(k, part):
        at = near[k]
        start, length = parts[part]
        found = jnp.dot(
            r.hot[at], r.dense[at, :, start : start + length], preferred_element_type=jnp.float32
        ).astype(jnp.bfloat16)
        r.aside[at, :, start : start + length] = found[SLOTS : 2 * SLOTS]
        across(at, part).start()
        r.packed[at, 0:SLOTS, start : start + length] = found[0:SLOTS]
        if part == 0:
            to_partner(at, 0).start()
        to_sibling(at, 0, part).start()

    def take_across(k, part):
        at = near[k]
        across(at, part).wait_recv()
        if part == 0:
            to_partner(at, 1).start()
        to_sibling(at, 1, part).start()

    def take_partner(k, half):
        to_partner(near[k], half).wait_recv()
        to_sibling(near[k], half, len(parts)).start()

    def get_ready(k):
        share_in(near[k] * 2 + x).wait_recv()
        prepare(near[k])

    def get_other_ready(k):
        share_in(near[k] * 2 + 1 - x).wait_recv()
        prepare_other(near[k])

    def active_copy(at):
        return copy(
            r.active.at[at, :, pl.ds(0, hidden)], r.active.at[at, :, pl.ds(hidden, hidden)],
            r.active_send, r.active_recv.at[at], sibling,
        )

    def enter(k):
        at = near[k]
        rows = pl.ds(0, 2 * SLOTS) if k else pl.ds(0, SLOTS)
        arrived = r.packed.at[at, rows, pl.ds(0, held + lone)]
        copy(arrived, arrived, r.core_send.at[at], r.core_recv.at[at], sibling).wait_recv()
        pre = jnp.dot(r.packed[at], r.both_weights[...], preferred_element_type=jnp.float32)
        gate_cut = jnp.minimum(pre[:, 0:hidden], CLAMP)
        up_pre = pre[:, hidden : 2 * hidden]
        r.active[at, :, 0:hidden] = (
            (jnp.clip(up_pre, -CLAMP, CLAMP) + 1.0) * gate_cut * jax.nn.sigmoid(SLOPE * gate_cut)
        ).astype(jnp.bfloat16)
        active_copy(at).start()

    late = quarter - early
    chunks = chunks_of(quarter, early)

    def pair_copy(at, half):
        return copy(
            r.results.at[at, rows_of(half), pl.ds(carried, early)], r.pair.at[at, rows_of(half), :],
            r.pair_send, r.pair_recv.at[at, half], partner,
        )

    def side_copy(at, chunk):
        start, length = chunks[chunk]
        return copy(
            r.results.at[at, rows_of(1), pl.ds(start, length)], r.side.at[at, :, pl.ds(start, length)],
            r.side_send, r.side_recv.at[at, chunk], beside,
        )

    def leave(k):
        at = near[k]
        active_copy(at).wait_recv()

        def finish(start, length):
            found = jnp.dot(
                r.active[at], r.down[:, start : start + length], preferred_element_type=jnp.float32
            )
            r.results[at, :, start : start + length] = (found * r.slot_weight[at][:, 0:1]).astype(
                jnp.bfloat16
            )

        for start in range(0, 2 * quarter, quarter // 2):
            finish(start, quarter // 2)

    def send_pair(k, half):
        pair_copy(near[k], half).start()

    def send_side(k):
        side_copy(near[k], 0).start()
        side_copy(near[k], 1).start()

    def take_pair(k, half):
        at = near[k]
        pair_copy(at, half).wait_recv()
        rows = slice(half * SLOTS, (half + 1) * SLOTS)
        for chunk in range(2, len(chunks)):
            columns = slice(chunks[chunk][0], chunks[chunk][0] + chunks[chunk][1])
            total = r.results[at, rows, columns].astype(jnp.float32)
            r.results[at, rows, columns] = (
                total + r.pair[at, rows, columns].astype(jnp.float32)
            ).astype(jnp.bfloat16)
            if half:
                side_copy(at, chunk).start()

    def line_copy(way, at, chunk):
        start, length = chunks[chunk]
        to = (jnp.where(at > z, e + 2, e - 2), t)
        return copy(
            r.line_out.at[at, :, pl.ds(start, length)], r.line_in.at[way, at, :, pl.ds(start, length)],
            r.line_send, r.line_recv.at[way, at, chunk], to,
        )

    last = copy(r.line_out.at[z, :, pl.ds(quarter, late)], r.last, r.last_send, r.last_recv, partner)

    def line_step(k, chunk, middle):
        at = near[k]
        start, length = chunks[chunk]
        columns = slice(start, start + length)
        side_copy(at, chunk).wait_recv()
        both_sides = jnp.concatenate([r.results[at, 0:SLOTS, columns], r.side[at, :, columns]], axis=0)
        total = lax.dot_general(
            r.hot[at], both_sides, (((0,), (0,)), ((), ())), preferred_element_type=jnp.float32
        )
        if k:
            way = jnp.where(at > z, 0, 1)
            ways = (way,) if middle else ()
        elif middle:
            ways = (0, 1)
        else:
            ways = (jnp.where(z == 0, 1, 0),)
        for way in ways:
            line_copy(way, at, chunk).wait_recv()
            total = total + r.line_in[way, at, :, columns].astype(jnp.float32)
        if k or chunk == 0:
            r.line_out[at, :, columns] = total.astype(jnp.bfloat16)
            if k:
                line_copy(way, at, chunk).start()
            else:
                last.start()
        elif chunk == 1:
            r.final[...] = total
        else:
            r.out[:, columns] = total.astype(jnp.bfloat16)

    def wait_expert_weights():
        pltpu.make_async_copy(r.both_weights, r.both_weights, r.load_sem.at[small + 1]).wait()

    def wait_down_weights():
        arrived = r.down.at[pl.ds(0, hidden)]
        pltpu.make_async_copy(arrived, arrived, r.load_sem.at[small + 2]).wait()
        copy(arrived, arrived, r.down_send, r.down_recv, sibling).wait_recv()

    def send_mixed(number):
        mixed_pair(number).start()

    def finish_mixed():
        whole = r.mixed_pair
        copy(whole, whole, r.mixed_pair_send, r.mixed_pair_recv, partner).wait_recv()
        total = r.mixed[mixed_rows(y), :].astype(jnp.float32)
        r.mixer[...] = (total + r.mixed_pair[...].astype(jnp.float32)).astype(jnp.bfloat16)

    def at_places(which, *steps):
        @pl.when(which)
        def _():
            for step in steps:
                step[0](*step[1:])

    def sent(view, semaphore):
        copy(view, view, semaphore, semaphore, sibling).wait_send()

    def drain_dispatch():
        @pl.when(z < LINE - 1)
        def _():
            sent(r.dense.at[0], r.own_send.at[1])

        @pl.when(z > 0)
        def _():
            sent(r.dense.at[0], r.own_send.at[0])

        @pl.when(at_middle)
        def _():
            sent(r.dense.at[pl.ds(0, LINE - 1)], r.onward_send)

        @pl.when(e < 2 * LINE - 1)
        def _():
            sent(r.halo, r.halo_send)

        sent(r.shares.at[pl.ds(0, 2 * LINE - 1)], r.share_send)
        sent(r.down.at[pl.ds(0, hidden)], r.down_send)
        sent(r.mixed_core, r.mixed_core_send)
        sent(r.aside, r.across_send)
        sent(r.active.at[:, :, pl.ds(0, hidden)], r.active_send)
        for k in range(LINE):
            at = near[k]
            rows = pl.ds(0, 2 * SLOTS) if k else pl.ds(0, SLOTS)
            sent(r.packed.at[at, rows, pl.ds(0, lone)], r.partner_send.at[at])
            sent(r.packed.at[at, rows, pl.ds(0, held + lone)], r.core_send.at[at])

    def drain_return():
        sent(r.mixed_pair, r.mixed_pair_send)
        sent(r.pair, r.pair_send)
        sent(r.side, r.side_send)

    at_places(
        at_end,
        (take_across, 0, 0),
        (take_end, 1, 0),
    )
    get_ready(1)
    at_places(
        at_middle,
        (forward, 2, 0),
        (forward, 1, 0),
    )
    attend(1, 0)
    at_places(at_end, (take_end, 1, 1))
    pack(1, 0)
    halo_wait()
    attend(0, 1)
    at_places(
        at_end,
        (take_across, 0, 2),
        (pack, 1, 1),
    )
    attend(1, 1)
    at_places(at_end, (take_partner, 0, 1))
    at_places(at_middle, (take_across, 0, 0))
    get_other_ready(0)
    attend(0, 0)
    at_places(at_end, (take_across, 1, 0))
    at_places(at_middle, (forward, 1, 1))
    get_ready(2)
    mix()
    at_places(at_end, (take_end, 2, 0))
    at_places(at_middle, (pack, 1, 1))
    pack(2, 0)
    at_places(
        at_middle,
        (take_across, 0, 2),
        (forward, 2, 1),
    )
    get_other_ready(1)
    at_places(at_end, (take_across, 0, 1))
    at_places(at_middle, (forward, 3, 0))
    get_ready(3)
    at_places(
        at_end,
        (take_partner, 1, 0),
        (take_end, 2, 1),
    )
    at_places(
        at_middle,
        (pack, 2, 1),
        (pack, 3, 0),
        (take_across, 0, 1),
        (forward, 2, 2),
    )
    mix_onward()
    at_places(
        at_end,
        (take_end, 1, 2),
        (send_mixed, 1),
        (pack, 1, 2),
    )
    at_places(
        at_middle,
        (forward, 3, 1),
        (take_across, 1, 1),
        (take_across, 1, 0),
        (pack, 2, 2),
        (take_partner, 0, 1),
        (take_across, 2, 0),
        (forward, 3, 2),
        (take_partner, 3, 0),
    )
    get_other_ready(2)
    at_places(at_middle, (take_across, 3, 0))
    get_other_ready(3)
    at_places(
        at_end,
        (take_end, 3, 0),
        (pack, 3, 0),
    )
    at_places(
        at_middle,
        (take_across, 2, 1),
        (take_partner, 1, 1),
        (forward, 1, 2),
        (send_mixed, 0),
        (pack, 3, 1),
    )
    wait_expert_weights()
    enter(0)
    at_places(
        at_end,
        (pack, 2, 1),
        (take_across, 2, 0),
        (take_across, 1, 1),
        (take_partner, 1, 1),
    )
    at_places(
        at_middle,
        (pack, 1, 2),
        (take_partner, 2, 0),
        (take_partner, 1, 0),
        (take_partner, 2, 1),
    )
    wait_down_weights()
    leave(0)
    at_places(
        at_middle,
        (take_across, 3, 1),
        (send_pair, 0, 1),
        (take_partner, 3, 1),
        (take_across, 2, 2),
        (pack, 3, 2),
        (send_side, 0),
        (send_pair, 0, 0),
    )
    take_across(1, 2)
    at_places(
        at_end,
        (take_end, 3, 1),
        (take_across, 3, 0),
        (send_mixed, 0),
        (pack, 3, 1),
        (take_partner, 3, 0),
        (take_end, 3, 2),
        (pack, 3, 2),
    )
    enter(1)
    at_places(at_end, (send_pair, 0, 0))
    at_places(at_middle, (take_across, 3, 2))
    leave(1)
    send_side(1)
    at_places(
        at_end,
        (take_across, 3, 1),
        (take_end, 2, 2),
    )
    send_pair(1, 1)
    at_places(
        at_end,
        (pack, 2, 2),
        (take_partner, 3, 1),
        (take_partner, 2, 1),
        (take_across, 3, 2),
    )
    enter(3)
    at_places(
        at_end,
        (take_partner, 2, 0),
        (take_across, 2, 1),
        (line_step, 1, 0, False),
    )
    at_places(at_middle, (send_pair, 1, 0))
    leave(3)
    send_side(3)
    at_places(
        at_end,
        (line_step, 1, 1, False),
        (send_pair, 3, 1),
    )
    at_places(at_middle, (take_pair, 0, 0))
    send_pair(3, 0)
    at_places(at_end, (take_across, 2, 2))
    enter(2)
    at_places(at_end, (line_step, 3, 0, False))
    leave(2)
    send_side(2)
    at_places(
        at_middle,
        (send_pair, 3, 1),
        (line_step, 3, 0, True),
        (take_pair, 3, 0),
        (send_pair, 2, 1),
        (line_step, 3, 1, True),
        (take_pair, 3, 1),
        (send_mixed, 2),
        (take_pair, 1, 0),
        (take_pair, 1, 1),
        (line_step, 2, 0, True),
        (line_step, 1, 0, True),
    )
    send_pair(2, 0)
    at_places(
        at_end,
        (line_step, 3, 1, False),
        (send_pair, 2, 1),
        (send_pair, 1, 0),
        (take_pair, 3, 1),
        (line_step, 2, 0, False),
        (take_pair, 3, 0),
        (take_pair, 0, 0),
        (line_step, 2, 1, False),
    )
    at_places(at_middle, (line_step, 1, 1, True))
    send_mixed(3)
    at_places(
        at_end,
        (send_pair, 0, 1),
        (send_mixed, 2),
        (line_step, 3, 2, False),
    )
    at_places(at_middle, (send_mixed, 1))
    take_pair(2, 1)
    at_places(
        at_end,
        (take_pair, 1, 1),
        (line_step, 3, 3, False),
    )
    at_places(
        at_middle,
        (line_step, 3, 2, True),
        (line_step, 2, 1, True),
        (take_pair, 0, 1),
        (line_step, 0, 0, True),
    )
    take_pair(2, 0)
    at_places(
        at_end,
        (take_pair, 1, 0),
        (line_step, 2, 2, False),
        (line_step, 2, 3, False),
        (send_side, 0),
        (line_step, 1, 2, False),
        (line_step, 1, 3, False),
        (take_pair, 0, 1),
        (line_step, 0, 0, False),
        (line_step, 0, 2, False),
    )
    at_places(
        at_middle,
        (line_step, 3, 3, True),
        (line_step, 0, 1, True),
        (line_step, 1, 2, True),
        (line_step, 2, 2, True),
    )
    drain_dispatch()
    at_places(at_end, (line_step, 0, 1, False))
    at_places(
        at_middle,
        (line_step, 1, 3, True),
        (line_step, 2, 3, True),
    )
    finish_mixed()
    at_places(at_end, (line_step, 0, 3, False))
    at_places(
        at_middle,
        (line_step, 0, 2, True),
        (line_step, 0, 3, True),
    )
    drain_return()

    last.wait_recv()
    r.out[:, early:quarter] = (r.final[...] + r.last[...].astype(jnp.float32)).astype(
        jnp.bfloat16
    )
    last.wait_send()
    sent(r.line_out.at[pl.ds(0, LINE - 1)], r.line_send)


def layer_call(
    rows, gain, routing, route_weight, queries, keys, values, sinks, project, gate_one, up_one, down_one
):
    tokens, width = rows.shape
    quarter, lone, both, early, carried = sizes_of(width)
    parts, chunks = len(parts_of(lone, both)), len(chunks_of(quarter, early))
    blocks = 2 * LINE
    hidden = gate_one.shape[1]
    kept = jnp.bfloat16
    dma = pltpu.SemaphoreType.DMA
    span = queries.shape[0] // 4
    stays = pl.BlockSpec(memory_space=pl.ANY)
    in_vmem = pl.BlockSpec(memory_space=pltpu.VMEM)
    scratch = dict(
        token=pltpu.VMEM(rows.shape, kept),
        gain=pltpu.VMEM(gain.shape, jnp.float32),
        routing=pltpu.VMEM(routing.shape, jnp.int32),
        route_weight=pltpu.VMEM(route_weight.shape, jnp.float32),
        query=pltpu.VMEM(queries.shape, kept),
        key=pltpu.VMEM(keys.shape, kept),
        value=pltpu.VMEM(values.shape, kept),
        sink=pltpu.SMEM(sinks.shape, jnp.float32),
        own=pltpu.VMEM((tokens, width), kept),
        dense=pltpu.VMEM((LINE, tokens, lone + both), kept),
        packed=pltpu.VMEM((LINE, 2 * SLOTS, width), kept),
        aside=pltpu.VMEM((LINE, SLOTS, lone + both), kept),
        both_weights=pltpu.VMEM((width, 2 * hidden), kept),
        down=pltpu.VMEM((2 * hidden, 2 * quarter), kept),
        project=pltpu.VMEM(project.shape, kept),
        halo=pltpu.VMEM((2, WINDOW_KEYS, keys.shape[1]), kept),
        attended=pltpu.VMEM(queries.shape, kept),
        mixed=pltpu.VMEM((queries.shape[0], width), kept),
        mixed_core=pltpu.VMEM((2, span, width), kept),
        mixed_pair=pltpu.VMEM((span, width), kept),
        shares=pltpu.VMEM((blocks, 8, tokens), jnp.float32),
        ranks=pltpu.VMEM((blocks, 8, tokens), jnp.float32),
        hot=pltpu.VMEM((LINE, 2 * SLOTS, tokens), kept),
        slot_weight=pltpu.VMEM((LINE, 2 * SLOTS, 128), jnp.float32),
        active=pltpu.VMEM((LINE, 2 * SLOTS, 2 * hidden), kept),
        results=pltpu.VMEM((LINE, 2 * SLOTS, 2 * quarter), kept),
        pair=pltpu.VMEM((LINE, 2 * SLOTS, early), kept),
        side=pltpu.VMEM((LINE, SLOTS, carried), kept),
        line_out=pltpu.VMEM((LINE, tokens, carried), kept),
        line_in=pltpu.VMEM((2, LINE, tokens, carried), kept),
        last=pltpu.VMEM((tokens, quarter - early), kept),
        final=pltpu.VMEM((tokens, quarter - early), jnp.float32),
        load_sem=dma((11,)),
        halo_send=dma,
        halo_recv=dma((2,)),
        mixed_core_send=dma,
        mixed_core_recv=dma((2,)),
        mixed_pair_send=dma,
        mixed_pair_recv=dma,
        share_send=dma,
        share_recv=dma((blocks,)),
        own_send=dma((2,)),
        onward_send=dma,
        along_recv=dma((LINE, parts)),
        across_send=dma,
        across_recv=dma((LINE, parts)),
        partner_send=dma((LINE,)),
        partner_recv=dma((LINE, 2)),
        core_send=dma((LINE,)),
        core_recv=dma((LINE,)),
        down_send=dma,
        down_recv=dma,
        active_send=dma,
        active_recv=dma((LINE,)),
        pair_send=dma,
        pair_recv=dma((LINE, 2)),
        side_send=dma,
        side_recv=dma((LINE, chunks)),
        line_send=dma,
        line_recv=dma((2, LINE, chunks)),
        last_send=dma,
        last_recv=dma,
    )
    return pl.pallas_call(
        layer_kernel,
        out_shape=(
            pltpu.VMEM((span, width), kept),
            pltpu.VMEM((tokens, quarter), kept),
        ),
        in_specs=[stays] * 12,
        out_specs=(in_vmem, in_vmem),
        scratch_shapes=[scratch[name] for name in NAMES[14:]],
        compiler_params=pltpu.CompilerParams(
            collective_id=0, has_side_effects=True, vmem_limit_bytes=60 * 1024 * 1024
        ),
        cost_estimate=pl.CostEstimate(
            flops=8 * blocks * tokens * width * hidden,
            bytes_accessed=8 * width * hidden,
            transcendentals=0,
        ),
    )(rows, gain, routing, route_weight, queries, keys, values, sinks, project, gate_one, up_one, down_one)


def shards(
    projected_queries,
    key_proj,
    projected_values,
    head_sink_logits,
    out_weight,
    expert_input,
    norm_gain,
    routing,
    route_weight,
    gate_weight,
    up_weight,
    down_weight,
):
    token_rows = expert_input.shape[0]
    experts = lax.axis_size("ep")
    capacity = max(3 * token_rows * TOPK // (2 * experts), 2)
    col_share = D // lax.axis_size("tp")
    if (experts, lax.axis_size("tp")) == (2 * LINE, 4) and token_rows == 128:
        return layer_call(
            expert_input,
            norm_gain[None, :],
            routing.T,
            route_weight.T,
            projected_queries,
            key_proj,
            projected_values,
            head_sink_logits,
            out_weight,
            gate_weight[0],
            up_weight[0],
            down_weight[0],
        )
    widened = expert_input.astype(jnp.float32)
    normed = (
        widened
        * lax.rsqrt(jnp.mean(widened * widened, axis=-1, keepdims=True) + EPS)
        * norm_gain[None, :]
    ).astype(jnp.bfloat16)
    query_rows = projected_queries.shape[0]
    kv_heads = key_proj.shape[1] // HEAD_SIZE
    heads_per_group = projected_queries.shape[1] // HEAD_SIZE // kv_heads
    count_of_blocks = query_rows // WINDOW_KEYS
    prior_key, prior_value = passed_along(
        (key_proj[query_rows - WINDOW_KEYS :], projected_values[query_rows - WINDOW_KEYS :]),
        "ep",
        1,
    )
    key_all = jnp.concatenate([prior_key, key_proj], axis=0)
    value_all = jnp.concatenate([prior_value, projected_values], axis=0)
    window_keys = jnp.concatenate(
        [
            key_all[:-WINDOW_KEYS].reshape(count_of_blocks, WINDOW_KEYS, kv_heads, HEAD_SIZE),
            key_all[WINDOW_KEYS:].reshape(count_of_blocks, WINDOW_KEYS, kv_heads, HEAD_SIZE),
        ],
        axis=1,
    )
    window_values = jnp.concatenate(
        [
            value_all[:-WINDOW_KEYS].reshape(count_of_blocks, WINDOW_KEYS, kv_heads, HEAD_SIZE),
            value_all[WINDOW_KEYS:].reshape(count_of_blocks, WINDOW_KEYS, kv_heads, HEAD_SIZE),
        ],
        axis=1,
    )
    query_blocks = projected_queries.reshape(
        count_of_blocks, WINDOW_KEYS, kv_heads, heads_per_group, HEAD_SIZE
    )
    scores = jnp.einsum(
        "nqhgd,nshd->nhgqs", query_blocks, window_keys, preferred_element_type=jnp.float32
    ) * HEAD_SIZE ** (-0.5)
    offset = lax.axis_index("ep") * query_rows
    block_ids = jnp.arange(count_of_blocks)[:, None, None] * WINDOW_KEYS + offset
    query_pos = block_ids + jnp.arange(WINDOW_KEYS)[None, :, None]
    key_pos = block_ids - WINDOW_KEYS + jnp.arange(2 * WINDOW_KEYS)[None, None, :]
    permitted_mask = (key_pos <= query_pos) & (query_pos - key_pos < WINDOW_KEYS) & (key_pos >= 0)
    scores = jnp.where(permitted_mask[:, None, None, :, :], scores, -jnp.inf)
    sink_col = head_sink_logits.reshape(kv_heads, heads_per_group)[None, :, :, None, None]
    highest = jnp.maximum(jnp.max(scores, axis=-1, keepdims=True), sink_col)
    numerator = jnp.exp(scores - highest)
    denominator = jnp.sum(numerator, axis=-1, keepdims=True) + jnp.exp(sink_col - highest)
    weights = (numerator / denominator).astype(jnp.bfloat16)
    attended = jnp.einsum(
        "nhgqs,nshd->nqhgd", weights, window_values, preferred_element_type=jnp.float32
    )
    attended = attended.astype(jnp.bfloat16).reshape(
        query_rows, kv_heads * heads_per_group * HEAD_SIZE
    )
    mixer_output = lax.psum_scatter(
        jnp.dot(attended, out_weight, preferred_element_type=jnp.float32).astype(jnp.bfloat16),
        "tp",
        scatter_dimension=0,
        tiled=True,
    )
    flat_ids = routing.reshape(-1)
    onehot = (flat_ids[:, None] == jnp.arange(experts, dtype=jnp.int32)[None, :]).astype(jnp.int32)
    rank_in = jnp.cumsum(onehot, axis=0) - 1
    target = flat_ids * capacity + jnp.sum(rank_in * onehot, axis=1)
    tok_ids = jnp.arange(token_rows * TOPK) // TOPK
    slot_tok = jnp.full((experts * capacity,), token_rows, jnp.int32).at[target].set(tok_ids)
    gate_one = gate_weight[0]
    up_one = up_weight[0]
    own_cols = lax.dynamic_slice_in_dim(normed, lax.axis_index("tp") * col_share, col_share, 1)
    extended = jnp.concatenate([own_cols, jnp.zeros((1, col_share), jnp.bfloat16)], axis=0)
    outgoing = jnp.take(extended, slot_tok, axis=0).reshape(experts, capacity, col_share)
    arrived = lax.all_to_all(outgoing, "ep", split_axis=0, concat_axis=0, tiled=True).reshape(
        experts * capacity, col_share
    )
    portion = lax.all_gather(arrived, "tp", axis=1, tiled=True)
    gate_pre = jnp.dot(portion, gate_one, preferred_element_type=jnp.float32)
    up_pre = jnp.dot(portion, up_one, preferred_element_type=jnp.float32)
    gate_cut = jnp.minimum(gate_pre, CLAMP)
    activated = (
        (jnp.clip(up_pre, -CLAMP, CLAMP) + 1.0) * gate_cut * jax.nn.sigmoid(SLOPE * gate_cut)
    ).astype(jnp.bfloat16)
    partial_value = jnp.dot(activated, down_weight[0], preferred_element_type=jnp.float32)
    expert_result = lax.psum_scatter(
        partial_value.astype(jnp.bfloat16), "tp", scatter_dimension=1, tiled=True
    )
    returned = lax.all_to_all(
        expert_result.reshape(experts, capacity, col_share),
        "ep",
        split_axis=0,
        concat_axis=0,
        tiled=True,
    )
    picked = jnp.take(returned.reshape(experts * capacity, col_share), target, axis=0)
    picked = picked.astype(jnp.float32).reshape(token_rows, TOPK, col_share)
    expert_output = jnp.sum(picked * route_weight[:, :, None], axis=1).astype(jnp.bfloat16)
    return (mixer_output, expert_output)


def solution(mesh):
    placed = (
        P("ep", "tp"),
        P("ep", "tp"),
        P("ep", "tp"),
        P("tp"),
        P("tp", None),
        P("ep", None),
        P(),
        P("ep", None),
        P("ep", None),
        P("ep", None, "tp"),
        P("ep", None, "tp"),
        P("ep", "tp", None),
    )
    return jax.shard_map(
        shards,
        mesh=mesh,
        in_specs=placed,
        out_specs=(P(("ep", "tp"), None), P("ep", "tp")),
        check_vma=False,
    )
```
